32 devices in a mesh: sp: 16 (over z, y, x), tp: 2 (over core).
Axes of the slice: x: 2, y: 2, z: 4, core: 2. Of those that a mesh axis runs over, the one named last changes fastest.
Arguments:
- tokens: bfloat16 [4096, 2048], P('sp', 'tp'), may hold values from -6 to 6
- norm_gain: float32 [2048], replicated, may hold values from 0.1 to 1.9
- glu_value: bfloat16 [2048, 2048], P('sp', 'tp'), may hold values from -0.125 to 0.125
- glu_gate: bfloat16 [2048, 2048], P('sp', 'tp'), may hold values from -0.125 to 0.125
- conv_taps: float32 [31, 2048], P(None, 'tp'), may hold values from -11 to 11
- ln_gain: float32 [2048], P('tp'), may hold values from 0.1 to 1.9
- ln_bias: float32 [2048], P('tp'), may hold values from -3 to 3
- query_weight: bfloat16 [2048, 2048], P('sp', 'tp'), may hold values from -0.125 to 0.125
- key_weight: bfloat16 [2048, 2048], P('sp', 'tp'), may hold values from -0.125 to 0.125
- value_weight: bfloat16 [2048, 2048], P('sp', 'tp'), may hold values from -0.125 to 0.125
- gate_weight: bfloat16 [2048, 32], replicated, may hold values from -0.125 to 0.125
- gate_bias: float32 [32], replicated, may hold values from -1 to 110
- log_decay_extra: float32 [4096, 16], P('sp'), may hold values from -1.3 to 0
- mem_gain: float32 [2048], P('tp'), may hold values from 0.1 to 1.9
- out_conv: bfloat16 [2048, 2048], P('tp'), may hold values from -0.125 to 0.125
- out_mem: bfloat16 [2048, 2048], P('tp'), may hold values from -0.125 to 0.125
Outputs:
- mixed: bfloat16 [4096, 2048], P(('sp', 'tp'))
The draws below stay inside these ranges and needn't reach their ends.
All inputs are finite; a program needn't handle non-finite values.
Results may differ from the reference program's by a relative error of at most 0.015.
Values may be sent and summed in bfloat16 or wider, within the bound.
No kernel may reach another device: no remote copies, remote signals or barrier semaphores. Data moves between devices by JAX's collectives and lax.ppermute only.
A program may use at most 128 MiB of HBM per device.

```python
import math
import jax
import jax.numpy as jnp
from jax import lax

D = 2048
CONV = 2048
MEMORY_HEADS = 8
HEAD = 256
KW = 31
BLOCK = 128
MEM = 2048
SEQUENCE_TOKENS = 4096
N_TP = 2


def draw_conv_taps(key, part):
    base_key, rough_key = jax.random.split(jax.random.fold_in(key, 11))
    base = jnp.clip(jax.random.normal(base_key, (KW, CONV), jnp.float32), -4.0, 4.0)
    rising = 10.0 ** (jnp.arange(CONV, dtype=jnp.float32) / CONV)
    rough = jax.random.uniform(rough_key, (1, CONV), jnp.float32, 0.5, 1.5)
    return base * rising[None, :] * rough * KW ** (-0.5)


def draw_gate_bias(key, part):
    input_key, pick_key, fast_key, slow_key = jax.random.split(jax.random.fold_in(key, 23), 4)
    inputs = jax.random.uniform(input_key, (2, MEMORY_HEADS), jnp.float32, -1.0, 1.0)
    share = 0.5
    fast = jax.random.uniform(pick_key, (2, MEMORY_HEADS), jnp.float32) < share
    fast_bias = jax.random.uniform(fast_key, (2, MEMORY_HEADS), jnp.float32, 3.4, 4.6)
    slow_bias = math.log(SEQUENCE_TOKENS) + 1.0 + jax.random.uniform(slow_key, (2, MEMORY_HEADS), jnp.float32, 0.0, 1.0)
    forget = jnp.where(fast, fast_bias, slow_bias)
    return jnp.stack([inputs[0], forget[0], inputs[1], forget[1]]).reshape(4 * MEMORY_HEADS)


def draw_log_decay_extra(key, part):
    rate_key, place_key, loss_key = jax.random.split(jax.random.fold_in(key, 37), 3)
    blocks = SEQUENCE_TOKENS // BLOCK
    rate_low = 0.25
    rate_high = 1.0
    rates = jnp.exp(jax.random.uniform(rate_key, (blocks, 2 * MEMORY_HEADS), jnp.float32, math.log(rate_low), math.log(rate_high)))
    stable_level = jnp.repeat(rates, BLOCK, axis=0) / SEQUENCE_TOKENS
    slot_places = jax.random.randint(place_key, (3, 2 * MEMORY_HEADS), 0, SEQUENCE_TOKENS)
    loss_values = jax.random.uniform(loss_key, (3, 2 * MEMORY_HEADS), jnp.float32, 0.22, 0.41)
    token_positions = jnp.arange(SEQUENCE_TOKENS, dtype=jnp.int32)[:, None]
    spike_values = jnp.zeros((SEQUENCE_TOKENS, 2 * MEMORY_HEADS), jnp.float32)
    for spike_value in range(3):
        spike_values = spike_values + jnp.where(token_positions == slot_places[spike_value][None, :], loss_values[spike_value][None, :], 0.0)
    return -(stable_level + spike_values)


def level_of(key, extent, cuts, smallest, high):
    gain = 1.0
    for axis_at, blocks in cuts:
        steps = jax.random.uniform(jax.random.fold_in(jax.random.fold_in(key, 6), axis_at), (blocks,), jnp.float32, smallest / len(cuts), high / len(cuts))
        gain = gain * jnp.repeat(jnp.exp(steps), extent[axis_at] // blocks).reshape((-1,) + (1,) * (len(extent) - 1 - axis_at))
    return gain


def gaussian(key, extent, spread, most, cuts=(), kind=jnp.bfloat16):
    array = jax.random.normal(key, extent, jnp.float32) * spread
    if len(cuts) > 0:
        array = level_of(key, extent, cuts, -0.22, 0.18) * array
    return jnp.clip(array, min=-most, max=most).astype(kind)


def setup_inputs(seed: int = 0) -> dict:
    seeds = jax.random.split(jax.random.key(seed), 17)
    return {
        "tokens": gaussian(seeds[0], (SEQUENCE_TOKENS, D), 1.0, 6.0, ((0, 16), (1, 2))),
        "norm_gain": jnp.clip(1.0 + 0.18 * jax.random.normal(seeds[1], (D,), jnp.float32), 0.1, 1.9),
        "glu_value": gaussian(seeds[2], (D, CONV), D ** -0.5, 0.125, ((0, 16), (1, 2))),
        "glu_gate": gaussian(seeds[3], (D, CONV), D ** -0.5, 0.125, ((0, 16), (1, 2))),
        "conv_taps": draw_conv_taps(jax.random.fold_in(seeds[16], 71), 0),
        "ln_gain": jnp.clip(1.0 + 0.18 * jax.random.normal(seeds[5], (CONV,), jnp.float32), 0.1, 1.9),
        "ln_bias": gaussian(seeds[6], (CONV,), 0.5, 3.0, ((0, 2),), jnp.float32),
        "query_weight": gaussian(seeds[7], (D, MEM), D ** -0.5, 0.125, ((0, 16), (1, 2))),
        "key_weight": gaussian(seeds[8], (D, MEM), D ** -0.5, 0.125, ((0, 16), (1, 2))),
        "value_weight": gaussian(seeds[9], (D, MEM), D ** -0.5, 0.125, ((0, 16), (1, 2))),
        "gate_weight": gaussian(seeds[10], (D, 4 * MEMORY_HEADS), D ** -0.5, 0.125),
        "gate_bias": draw_gate_bias(jax.random.fold_in(seeds[16], 71), 0),
        "log_decay_extra": draw_log_decay_extra(jax.random.fold_in(seeds[16], 71), 0),
        "mem_gain": jnp.clip(1.0 + 0.18 * jax.random.normal(seeds[13], (MEM,), jnp.float32), 0.1, 1.9),
        "out_conv": gaussian(seeds[14], (CONV, D), CONV ** -0.5, 0.125, ((0, 2),)),
        "out_mem": gaussian(seeds[15], (MEM, D), MEM ** -0.5, 0.125, ((0, 2),)),
    }


EPS = 1e-06
LOW_START = -1e+30
PRECISE = lax.Precision.HIGHEST

def block_step(carried_state, block_data):
    state_mat, state_vec, stabilizer = carried_state
    queries, key_rows, value_rows, input_gate, log_forget = block_data
    key_scale = HEAD ** (-0.5)
    length = log_forget.shape[-1]
    causal = jnp.tril(jnp.ones((length, length), dtype=bool))
    decay_sum = jnp.cumsum(log_forget, axis=-1)
    log_weight = jnp.where(causal, decay_sum[:, :, None] - decay_sum[:, None, :] + input_gate[:, None, :], -jnp.inf)
    carried = decay_sum + stabilizer[:, None]
    running = jnp.maximum(carried, lax.optimization_barrier(jnp.max(log_weight, axis=-1)))
    inner_weight = jnp.exp(log_weight - running[:, :, None])
    carry_weight = jnp.exp(carried - running)
    raw_scores = jnp.einsum('htd,hsd->hts', queries, key_rows, preferred_element_type=jnp.float32)
    scores = raw_scores * key_scale * inner_weight
    query_wide = queries.astype(jnp.float32)
    numerator = carry_weight[:, :, None] * jnp.einsum('htd,hde->hte', query_wide, state_mat, precision=PRECISE)
    numerator = numerator + jnp.einsum('hts,hse->hte', scores.astype(jnp.bfloat16), value_rows, preferred_element_type=jnp.float32)
    denominator = carry_weight * jnp.einsum('htd,hd->ht', query_wide, state_vec, precision=PRECISE) + lax.optimization_barrier(jnp.sum(scores, axis=-1))
    to_end = decay_sum[:, -1:] - decay_sum + input_gate
    carried_end = decay_sum[:, -1] + stabilizer
    new_stabilizer = jnp.maximum(carried_end, lax.optimization_barrier(jnp.max(to_end, axis=-1)))
    end_weight = jnp.exp(to_end - new_stabilizer[:, None]) * key_scale
    keep_weight = jnp.exp(carried_end - new_stabilizer)
    weighted = key_rows.astype(jnp.float32) * end_weight[:, :, None]
    new_mat = keep_weight[:, None, None] * state_mat + jnp.einsum('hsd,hse->hde', weighted.astype(jnp.bfloat16), value_rows, preferred_element_type=jnp.float32)
    new_vec = keep_weight[:, None] * state_vec + lax.optimization_barrier(jnp.sum(weighted, axis=1))
    return ((new_mat, new_vec, new_stabilizer), (numerator, denominator, running, decay_sum))

def one_direction(queries, key_proj, value_proj, input_gate, log_forget):
    count = SEQUENCE_TOKENS // BLOCK

    def heads_first(tensor):
        return jnp.transpose(tensor.reshape(BLOCK, MEMORY_HEADS, HEAD), (1, 0, 2))

    def step(carried_state, block_data):
        query_blk, key_blk, value_blk, input_blk, forget_blk = block_data
        new_state, results = block_step(carried_state, (heads_first(query_blk), heads_first(key_blk), heads_first(value_blk), input_blk.T, forget_blk.T))
        numerator, denominator, running, _ = results
        return (new_state, numerator / jnp.maximum(jnp.abs(denominator), jnp.exp(-running))[:, :, None])
    start = (jnp.zeros((MEMORY_HEADS, HEAD, HEAD), jnp.float32), jnp.zeros((MEMORY_HEADS, HEAD), jnp.float32), jnp.full((MEMORY_HEADS,), LOW_START, jnp.float32))
    inputs = (queries.reshape(count, BLOCK, MEM), key_proj.reshape(count, BLOCK, MEM), value_proj.reshape(count, BLOCK, MEM), input_gate.reshape(count, BLOCK, MEMORY_HEADS), log_forget.reshape(count, BLOCK, MEMORY_HEADS))
    _, outputs = lax.scan(step, start, inputs)
    return jnp.transpose(outputs, (0, 2, 1, 3)).reshape(SEQUENCE_TOKENS, MEMORY_HEADS, HEAD)

def reference(tokens, norm_gain, glu_value, glu_gate, conv_taps, ln_gain, ln_bias, query_weight, key_weight, value_weight, gate_weight, gate_bias, log_decay_extra, mem_gain, out_conv, out_mem):
    wide = tokens.astype(jnp.float32)
    normed = (wide * lax.rsqrt(lax.optimization_barrier(jnp.mean(wide * wide, axis=-1, keepdims=True)) + EPS) * norm_gain).astype(jnp.bfloat16)
    value_sum = jnp.dot(normed, glu_value, preferred_element_type=jnp.float32)
    gate_sum = jnp.dot(normed, glu_gate, preferred_element_type=jnp.float32)
    glu = (value_sum * jax.nn.sigmoid(gate_sum)).astype(jnp.bfloat16)
    reach = KW // 2
    padded = jnp.pad(glu.astype(jnp.float32), ((reach, reach), (0, 0)))
    conv = jnp.zeros((SEQUENCE_TOKENS, CONV), jnp.float32)
    for offset in range(KW):
        conv = conv + conv_taps[offset] * padded[offset:offset + SEQUENCE_TOKENS]
    chan_mean = lax.optimization_barrier(jnp.mean(conv, axis=-1, keepdims=True))
    chan_var = lax.optimization_barrier(jnp.mean(conv * conv, axis=-1, keepdims=True)) - chan_mean * chan_mean
    normal = (conv - chan_mean) * lax.rsqrt(chan_var + EPS) * ln_gain + ln_bias
    act = (normal * jax.nn.sigmoid(normal)).astype(jnp.bfloat16)
    queries = jnp.dot(normed, query_weight, preferred_element_type=jnp.float32).astype(jnp.bfloat16)
    key_proj = jnp.dot(normed, key_weight, preferred_element_type=jnp.float32).astype(jnp.bfloat16)
    value_proj = jnp.dot(normed, value_weight, preferred_element_type=jnp.float32).astype(jnp.bfloat16)
    gates = (jnp.dot(normed, gate_weight, preferred_element_type=jnp.float32) + gate_bias).reshape(SEQUENCE_TOKENS, 4, MEMORY_HEADS)
    extra = log_decay_extra.reshape(SEQUENCE_TOKENS, 2, MEMORY_HEADS)
    forget_fwd = jax.nn.log_sigmoid(gates[:, 1]) + extra[:, 0]
    forget_bwd = jax.nn.log_sigmoid(gates[:, 3]) + extra[:, 1]
    forward_out = one_direction(queries, key_proj, value_proj, gates[:, 0], forget_fwd)
    backward_out = jnp.flip(one_direction(jnp.flip(queries, 0), jnp.flip(key_proj, 0), jnp.flip(value_proj, 0), jnp.flip(gates[:, 2], 0), jnp.flip(forget_bwd, 0)), 0)
    summed = forward_out + backward_out
    head_norm = summed * lax.rsqrt(lax.optimization_barrier(jnp.mean(summed * summed, axis=-1, keepdims=True)) + EPS)
    memory = (head_norm * mem_gain.reshape(MEMORY_HEADS, HEAD)).reshape(SEQUENCE_TOKENS, MEM).astype(jnp.bfloat16)
    conv_group = CONV // N_TP
    mem_group = MEM // N_TP
    total = jnp.zeros((SEQUENCE_TOKENS, D), jnp.float32)
    for channel_group in range(N_TP):
        conv_cols = act[:, channel_group * conv_group:(channel_group + 1) * conv_group]
        mem_cols = memory[:, channel_group * mem_group:(channel_group + 1) * mem_group]
        partial_sum = jnp.dot(conv_cols, out_conv[channel_group * conv_group:(channel_group + 1) * conv_group], preferred_element_type=jnp.float32)
        partial_sum = partial_sum + jnp.dot(mem_cols, out_mem[channel_group * mem_group:(channel_group + 1) * mem_group], preferred_element_type=jnp.float32)
        total = total + lax.optimization_barrier(partial_sum.astype(jnp.bfloat16)).astype(jnp.float32)
    return total.astype(jnp.bfloat16)
```

```python
import functools
import jax
import jax.numpy as jnp
from jax import lax
from jax.experimental import pallas as pl
from jax.experimental.pallas import tpu as pltpu
from jax.sharding import PartitionSpec as P

MEMORY_HEADS = 8
HEAD = 256
KW = 31
REACH = KW // 2
HALO = 16
TAIL = 16

EPS = 1e-06
LOW_START = -1e30
RING_MOST = 8
F32 = jnp.float32
BF16 = jnp.bfloat16


def params(**kw):
    return pltpu.CompilerParams(vmem_limit_bytes=56 * 1024 * 1024, **kw)


def whole(shape):
    return pl.BlockSpec(shape, lambda i, tab: (0,) * len(shape))


def dot(a, b):
    return jnp.dot(a, b, preferred_element_type=F32)


def dot_nt(a, b, **kw):
    return lax.dot_general(a, b, (((1,), (1,)), ((), ())), preferred_element_type=F32, **kw)


def dot_tn(a, b):
    return lax.dot_general(a, b, (((0,), (0,)), ((), ())), preferred_element_type=F32)


def scan_lanes(x, op, identity, reverse):
    width = x.shape[1]
    lane = lax.broadcasted_iota(jnp.int32, x.shape, 1)
    step = 1
    while step < width:
        if reverse:
            moved = pltpu.roll(x, width - step, 1)
            keep = lane < width - step
        else:
            moved = pltpu.roll(x, step, 1)
            keep = lane >= step
        x = op(x, jnp.where(keep, moved, identity))
        step *= 2
    return x


def log_sigmoid(x):
    return jnp.minimum(x, 0.0) - jnp.log1p(jnp.exp(-jnp.abs(x)))


def split3(x):
    high = x.astype(BF16)
    rest = x - high.astype(F32)
    mid = rest.astype(BF16)
    low = (rest - mid.astype(F32)).astype(BF16)
    return high.astype(F32), mid.astype(F32), low.astype(F32)


def assemble(tab, first, blocks, rows, pieces, scratch):
    per = pieces[0].shape[0] // rows
    for block in range(blocks):
        start = pl.multiple_of(tab[first + block], rows)
        slot = (block % per) * rows
        scratch[pl.ds(start, rows), :] = pieces[block // per][slot : slot + rows, :]


def project(parts, weights):
    total = None
    for place, part in enumerate(parts):
        wide = part.shape[1]
        term = dot(part, weights[place * wide : (place + 1) * wide, :])
        total = term if total is None else total + term
    return total


def keys_kernel(dims, tab, *refs):
    group, blocks, rows, n_parts, n_pieces, key_scale = dims
    refs = list(refs)
    parts = [refs.pop(0) for _ in range(n_parts)]
    key_pieces = [refs.pop(0) for _ in range(n_pieces)]
    value_pieces = [refs.pop(0) for _ in range(n_pieces)]
    gate_rows, gate_bias, extra = refs.pop(0), refs.pop(0), refs.pop(0)
    key_out, value_out, rows_out, fwd_out, bwd_out = refs[:5]
    key_w, value_w, gates, extras = refs[5:]
    step = pl.program_id(0)
    count = extra.shape[2]

    @pl.when(step == 0)
    def _():
        assemble(tab, 3 * group + 1, blocks, rows, key_pieces, key_w)
        assemble(tab, 3 * group + 1, blocks, rows, value_pieces, value_w)

    here = pl.ds(pl.multiple_of(step * count, count), count)
    held = [part[...] for part in parts]
    key_out[here, :] = project(held, key_w).astype(BF16)
    value_out[here, :] = project(held, value_w).astype(BF16)
    pre = gate_bias[:, 0:1]
    for place, part in enumerate(held):
        wide = part.shape[1]
        pre = pre + dot_nt(gate_rows[:, place * wide : (place + 1) * wide], part)
    gates[:, here] = pre[0:8, :]
    extras[:, here] = extra[0]

    @pl.when(step == group - 1)
    def _():
        pre = gates[...]
        more = extras[...]
        in_f, in_b = pre[0:1, :], pre[2:3, :]
        forget_f = log_sigmoid(pre[1:2, :]) + more[0:1, :]
        forget_b = log_sigmoid(pre[3:4, :]) + more[1:2, :]
        width = pre.shape[1]
        sub = lax.broadcasted_iota(jnp.int32, (8, width), 0)
        decay_f = scan_lanes(jnp.broadcast_to(forget_f, (8, width)), jnp.add, 0.0, False)[0:1]
        decay_b = scan_lanes(jnp.broadcast_to(forget_b, (8, width)), jnp.add, 0.0, True)[0:1]
        level_f, level_b = in_f - decay_f, in_b - decay_b
        peak_f = scan_lanes(jnp.broadcast_to(level_f, (8, width)), jnp.maximum, LOW_START, False)[0:1]
        peak_b = scan_lanes(jnp.broadcast_to(level_b, (8, width)), jnp.maximum, LOW_START, True)[0:1]
        most_f = jnp.max(level_f, axis=1, keepdims=True)
        most_b = jnp.max(level_b, axis=1, keepdims=True)
        vectors = [level_f, level_b, decay_f, decay_b, peak_f, peak_b]
        table = jnp.zeros((8, width), F32)
        for place, vector in enumerate(vectors):
            table = jnp.where(sub == place, vector, table)
        rows_out[...] = table
        weights = jnp.where(sub == 0, jnp.exp(level_f - most_f), jnp.exp(level_b - most_b)) * key_scale
        columns = jnp.transpose(weights)
        keys = key_out[...].astype(F32)
        values = value_out[...]
        ends = ((fwd_out, 0, decay_f[:, width - 1 :], most_f), (bwd_out, 1, decay_b[:, 0:1], most_b))
        for out, place, total, most in ends:
            weighted = keys * columns[:, place : place + 1]
            mat = dot_tn(weighted.astype(BF16), values)
            vec = jnp.sum(weighted, axis=0, keepdims=True)
            out[0:HEAD, :] = mat.astype(BF16)
            lines = (*split3(vec), *split3(total), *split3(total + most))
            at = lax.broadcasted_iota(jnp.int32, (TAIL, HEAD), 0)
            tail = jnp.zeros((TAIL, HEAD), F32)
            for line, value in enumerate(lines):
                tail = jnp.where(at == line, value, tail)
            out[HEAD:, :] = tail.astype(BF16)


def glu_kernel(dims, tab, *refs):
    group, blocks, rows, n_parts, n_pieces = dims
    refs = list(refs)
    parts = [refs.pop(0) for _ in range(n_parts)]
    value_pieces = [refs.pop(0) for _ in range(n_pieces)]
    gate_pieces = [refs.pop(0) for _ in range(n_pieces)]
    glu_out, head_out, tail_out, value_w, gate_w = refs
    step = pl.program_id(0)

    @pl.when(step == 0)
    def _():
        assemble(tab, 3 * group + 1, blocks, rows, value_pieces, value_w)
        assemble(tab, 3 * group + 1, blocks, rows, gate_pieces, gate_w)

    held = [part[...] for part in parts]
    glu = (project(held, value_w) * jax.nn.sigmoid(project(held, gate_w))).astype(BF16)
    glu_out[...] = glu

    @pl.when(step == 0)
    def _():
        head_out[...] = glu[0:HALO, :]

    @pl.when(step == group - 1)
    def _():
        tail_out[...] = glu[glu.shape[0] - HALO :, :]


def conv_kernel(glu, before, after, taps, conv_out, stats_out, padded):
    length, width = glu.shape
    padded[0:HALO, :] = before[...].astype(F32)
    padded[HALO : HALO + length, :] = glu[...].astype(F32)
    padded[HALO + length :, :] = after[...].astype(F32)
    chunk = 64
    lead = HALO - REACH

    def one(step, carry):
        base = pl.multiple_of(step * chunk, chunk)
        total = jnp.zeros((chunk, width), F32)
        window_all = padded[pl.ds(base, chunk + 32), :]
        for shift in range(8):
            window = pltpu.roll(window_all, chunk + 32 - shift, 0) if shift else window_all
            for high in range(4):
                tap = 8 * high + shift - lead
                if 0 <= tap < KW:
                    total = total + taps[tap : tap + 1, :] * window[8 * high : 8 * high + chunk, :]
        conv_out[pl.ds(base, chunk), :] = total
        return carry

    lax.fori_loop(0, length // chunk, one, 0)
    conv = conv_out[...]
    ones = jnp.ones((8, width), F32)
    sums = dot_nt(ones, conv, precision=lax.Precision.HIGHEST)
    squares = dot_nt(ones, conv * conv, precision=lax.Precision.HIGHEST)
    sub = lax.broadcasted_iota(jnp.int32, sums.shape, 0)
    stats_out[...] = jnp.where(sub == 0, sums, squares)


def act_kernel(dims, tab, conv, *refs):
    group, channels = dims
    stats, (gain, bias), outs = refs[:group], refs[group : group + 2], refs[group + 2 :]
    total = stats[0][...]
    for more in stats[1:]:
        total = total + more[...]
    mean = total[0:1, :] / channels
    var = total[1:2, :] / channels - mean * mean
    scale = lax.rsqrt(var + EPS)
    sub = lax.broadcasted_iota(jnp.int32, total.shape, 0)
    columns = jnp.transpose(jnp.where(sub == 0, mean, scale))
    count = outs[0].shape[0]
    for slot, out in enumerate(outs):
        start = pl.multiple_of(tab[group + slot] * count, count)
        normal = (conv[pl.ds(start, count), :] - columns_at(columns, 0, tab[group + slot], group, count)) * columns_at(
            columns, 1, tab[group + slot], group, count
        )
        normal = normal * gain[...] + bias[...]
        out[...] = (normal * jax.nn.sigmoid(normal)).astype(BF16)


def columns_at(columns, lane, which, group, count):
    out = columns[0:count, lane : lane + 1]
    for block in range(1, group):
        out = jnp.where(which == block, columns[block * count : (block + 1) * count, lane : lane + 1], out)
    return out


def incoming(tab, place, group, pieces, spot, reverse, sizes):
    at = tab[3 * group]
    levels, best, passed = [], jnp.full((1, HEAD), LOW_START, F32), jnp.zeros((1, HEAD), F32)
    for hop, piece in enumerate(pieces):
        lines = piece[HEAD:, :].astype(F32)
        total = lines[3:4] + lines[4:5] + lines[5:6]
        level = lines[6:7] + lines[7:8] + lines[8:9] + passed
        there = (at + hop + 1 < sizes) if reverse else (at - hop - 1 >= 0)
        level = jnp.where(there, level, LOW_START)
        levels.append(level)
        best = jnp.maximum(best, level)
        passed = passed + total
    mat = jnp.zeros((HEAD, HEAD), F32)
    vec = jnp.zeros((1, HEAD), F32)
    for piece, level in zip(pieces, levels):
        weight = jnp.exp(level - best)
        lines = piece[HEAD:, :].astype(F32)
        mat = mat + weight * piece[0:HEAD, :].astype(F32)
        vec = vec + weight * (lines[0:1] + lines[1:2] + lines[2:3])
    return mat, vec, best


def memory_kernel(dims, tab, *refs):
    group, blocks, rows, n_parts, n_pieces, n_states, quarters, key_scale = dims
    refs = list(refs)
    parts = [refs.pop(0) for _ in range(n_parts)]
    pieces = [refs.pop(0) for _ in range(n_pieces)]
    keys, values, table, table_block = refs.pop(0), refs.pop(0), refs.pop(0), refs.pop(0)
    key_block, value_block = refs.pop(0), refs.pop(0)
    before = [refs.pop(0) for _ in range(n_states)]
    after = [refs.pop(0) for _ in range(n_states)]
    gain = refs.pop(0)
    outs = [refs.pop(0) for _ in range(group)]
    query_w, mats_hi, mats_lo, vecs = refs
    step = pl.program_id(0)

    @pl.when(step == 0)
    def _():
        assemble(tab, 3 * group + 1, blocks, rows, pieces, query_w)
        for spot, states in enumerate((before, after)):
            mat, vec, best = incoming(tab, spot, group, states, spot, spot == 1, quarters)
            high = mat.astype(BF16)
            mats_hi[spot] = high
            mats_lo[spot] = (mat - high.astype(F32)).astype(BF16)
            vecs[2 * spot : 2 * spot + 1, :] = vec
            vecs[2 * spot + 1 : 2 * spot + 2, :] = best

    held = [part[...] for part in parts]
    queries = project(held, query_w).astype(BF16)
    wide = queries.astype(F32)
    count = queries.shape[0]
    length = keys.shape[0]
    columns = jnp.transpose(table_block[...])
    raw = dot_nt(queries, keys[...]) * key_scale
    spot_t = step * count + lax.broadcasted_iota(jnp.int32, (count, length), 0)
    spot_s = lax.broadcasted_iota(jnp.int32, (count, length), 1)
    best_f, best_b = vecs[1:2, 0:1], vecs[3:4, 0:1]
    top_f = jnp.maximum(columns[:, 4:5], best_f)
    top_b = jnp.maximum(columns[:, 5:6], best_b)
    early = spot_s <= spot_t
    power = jnp.where(early, table[0:1, :] - top_f, table[1:2, :] - top_b)
    scores = raw * jnp.exp(power)
    scores_f = jnp.where(early, scores, 0.0)
    scores_b = jnp.where(early, 0.0, scores)
    own = jnp.sum(wide * key_block[...].astype(F32), axis=1, keepdims=True) * key_scale
    own = own * jnp.exp(columns[:, 1:2] - top_b)
    carry_f, carry_b = jnp.exp(best_f - top_f), jnp.exp(best_b - top_b)
    numer_f = dot(scores_f.astype(BF16), values[...])
    numer_b = dot(scores_b.astype(BF16), values[...])
    numer_b = numer_b + own.astype(BF16).astype(F32) * value_block[...].astype(F32)
    numer_f = numer_f + carry_f * (dot(queries, mats_hi[0]) + dot(queries, mats_lo[0]))
    numer_b = numer_b + carry_b * (dot(queries, mats_hi[1]) + dot(queries, mats_lo[1]))
    denom_f = jnp.sum(scores_f, axis=1, keepdims=True)
    denom_b = jnp.sum(scores_b, axis=1, keepdims=True) + own
    denom_f = denom_f + carry_f * jnp.sum(wide * vecs[0:1, :], axis=1, keepdims=True)
    denom_b = denom_b + carry_b * jnp.sum(wide * vecs[2:3, :], axis=1, keepdims=True)
    floor_f = jnp.exp(-(columns[:, 2:3] + top_f))
    floor_b = jnp.exp(-(columns[:, 3:4] + top_b))
    summed = numer_f / jnp.maximum(jnp.abs(denom_f), floor_f)
    summed = summed + numer_b / jnp.maximum(jnp.abs(denom_b), floor_b)
    scale = lax.rsqrt(jnp.mean(summed * summed, axis=1, keepdims=True) + EPS)
    result = (summed * scale * gain[...]).astype(BF16)
    for slot, out in enumerate(outs):

        @pl.when(tab[group + slot] == step)
        def _():
            out[...] = result


def out_kernel(dims, tab, *refs):
    group, halves = dims
    acts, mems = refs[:group], refs[group : 2 * group]
    out_conv, out_mem = refs[2 * group : 2 * group + 2]
    outs = refs[2 * group + 2 : 2 * group + 2 + halves]
    total = refs[-1]
    for slot in range(group):
        wide = acts[slot].shape[1]
        rows = pl.ds(pl.multiple_of(tab[slot] * wide, wide), wide)
        term = dot(acts[slot][...], out_conv[rows, :])
        wide = mems[slot].shape[1]
        rows = pl.ds(pl.multiple_of(tab[slot] * wide, wide), wide)
        term = term + dot(mems[slot][...], out_mem[rows, :])
        total[...] = term if slot == 0 else total[...] + term
    if halves == 1:
        outs[0][...] = total[...].astype(BF16)
    else:
        half = outs[0].shape[0]
        own = tab[2 * group]
        outs[0][...] = total[pl.ds(pl.multiple_of(own * half, half), half), :].astype(BF16)
        outs[1][...] = total[pl.ds(pl.multiple_of((1 - own) * half, half), half), :].astype(BF16)


def compose_line(total, level, mat, vec):
    tail = jnp.concatenate([jnp.broadcast_to(x[None, :], (1, HEAD)) for x in (*split3(vec), *split3(total + jnp.zeros((HEAD,), F32)), *split3(level + jnp.zeros((HEAD,), F32)))])
    tail = jnp.concatenate([tail, jnp.zeros((TAIL - tail.shape[0], HEAD), F32)])
    return jnp.concatenate([mat, tail]).astype(BF16)


def shards(
    tokens,
    norm_gain,
    glu_value,
    glu_gate,
    conv_taps,
    ln_gain,
    ln_bias,
    query_weight,
    key_weight,
    value_weight,
    gate_weight,
    gate_bias,
    log_decay_extra,
    mem_gain,
    out_conv,
    out_mem,
):
    sp, tp = lax.axis_size("sp"), lax.axis_size("tp")
    group = mem_gain.shape[0] // HEAD
    quarters = sp // group
    count = tokens.shape[0]
    length = group * count
    rows = key_weight.shape[0]
    features = norm_gain.shape[0]
    channels = conv_taps.shape[1] // group
    conv_all = channels * group * tp
    blocks = sp
    key_scale = HEAD ** (-0.5)
    me, core = lax.axis_index("sp"), lax.axis_index("tp")
    place, quarter = me % group, me // group
    paired = tp == 2
    even = group & (group - 1) == 0
    ringed = quarters <= RING_MOST

    def source(p, slot):
        return p ^ slot if even else (p - slot) % group

    def target(p, slot):
        return p ^ slot if even else (p + slot) % group

    def in_plane(x, slot):
        if slot == 0:
            return x
        return lax.ppermute(x, "sp", [(i, i - i % group + target(i % group, slot)) for i in range(sp)])

    def along(x, hops, ring=False):
        pairs = [(i, i + hops * group) for i in range(sp)]
        pairs = [(i, j % sp) for i, j in pairs] if ring else [(i, j) for i, j in pairs if 0 <= j < sp]
        return lax.ppermute(x, "sp", pairs)

    def swap(x):
        return lax.ppermute(x, "tp", [(0, 1), (1, 0)])

    lines = [[k * group + j for k in range(quarters)] for j in range(group)]

    def tall(x):
        return jnp.concatenate(x, axis=0) if len(x) > 1 else x[0]

    def gather_weight(weight, width):
        sent = [
            lax.dynamic_slice_in_dim(weight, target(place, slot) * width, width, 1) for slot in range(group)
        ]
        piece = tall([in_plane(x, slot) for slot, x in enumerate(sent)])
        if not ringed:
            return [lax.all_gather(piece, "sp", axis=0, tiled=True, axis_index_groups=lines)]
        pieces = [piece]
        for _ in range(quarters - 1):
            pieces.append(along(pieces[-1], 1, True))
        return pieces

    slots = list(range(group))
    sources = [source(place, slot) for slot in slots]
    targets = [target(place, slot) for slot in slots]
    inverse = [p ^ place if even else (place - p) % group for p in slots]
    shift = core * tokens.shape[1] if paired else 0
    offsets = []
    for hop in range(quarters):
        block_quarter = (quarter - hop) % quarters if ringed else hop
        for slot in slots:
            offsets.append(((block_quarter * group + sources[slot]) * rows - shift) % features)
    tab = jnp.stack([jnp.asarray(x, jnp.int32) for x in (*sources, *targets, *inverse, quarter, *offsets)])
    out_tab = jnp.stack([jnp.asarray(x, jnp.int32) for x in (*sources, *targets, core)])

    key_pieces = gather_weight(key_weight, HEAD)
    wide = tokens.astype(F32)
    squares = jnp.sum(wide * wide, axis=-1, keepdims=True)
    squares = squares + swap(squares) if paired else lax.psum(squares, "tp")
    own_gain = lax.dynamic_slice_in_dim(norm_gain, core * tokens.shape[1], tokens.shape[1], 0)
    normed = (wide * lax.rsqrt(squares / features + EPS) * own_gain).astype(BF16)
    normed = tall([in_plane(normed, slot) for slot in slots])
    parts = [normed, swap(normed)] if paired else [lax.all_gather(normed, "tp", axis=1, tiled=True)]
    head = core * group + place
    extra = lax.dynamic_slice_in_dim(log_decay_extra.T.reshape(2, MEMORY_HEADS, count), 0, 2, 0)
    extra = jnp.concatenate([extra.reshape(2 * MEMORY_HEADS, count)], 0)
    extra_pieces = [in_plane(extra, slot) for slot in slots]
    extra = jnp.stack(extra_pieces).reshape(group, 2, MEMORY_HEADS, count)
    extra = lax.dynamic_slice_in_dim(extra, head, 1, 2)[:, :, 0]
    extra = jnp.pad(extra, ((0, 0), (0, 6), (0, 0)))
    gate_rows = lax.dynamic_slice_in_dim(gate_weight.reshape(features, 4, MEMORY_HEADS), head, 1, 2)[:, :, 0].T
    if paired:
        gate_rows = jnp.where(core == 0, gate_rows, jnp.roll(gate_rows, features // 2, 1))
    gate_rows = jnp.pad(gate_rows, ((0, 12), (0, 0)))
    bias = lax.dynamic_slice_in_dim(gate_bias.reshape(4, MEMORY_HEADS), head, 1, 1)
    bias = jnp.pad(jnp.broadcast_to(bias, (4, 128)), ((0, 12), (0, 0)))

    value_pieces = gather_weight(value_weight, HEAD)
    glu_pieces = gather_weight(glu_value, channels)
    gate_pieces = gather_weight(glu_gate, channels)
    query_pieces = gather_weight(query_weight, HEAD)
    n_parts, n_pieces = len(parts), len(key_pieces)

    def part_specs():
        return [
            pl.BlockSpec((count, part.shape[1]), lambda i, tab: (tab[2 * group + i], 0)) for part in parts
        ]

    def piece_specs(width):
        return [whole((piece.shape[0], width)) for piece in key_pieces]

    state_shape = jax.ShapeDtypeStruct((HEAD + TAIL, HEAD), BF16)
    keys, values, table, state_f, state_b = pl.pallas_call(
        functools.partial(keys_kernel, (group, blocks, rows, n_parts, n_pieces, key_scale)),
        grid_spec=pltpu.PrefetchScalarGridSpec(
            num_scalar_prefetch=1,
            grid=(group,),
            in_specs=part_specs()
            + piece_specs(HEAD) * 2
            + [
                whole((16, features)),
                whole((16, 128)),
                pl.BlockSpec((1, 8, count), lambda i, tab: (tab[2 * group + i], 0, 0)),
            ],
            out_specs=[
                whole((length, HEAD)),
                whole((length, HEAD)),
                whole((8, length)),
                whole((HEAD + TAIL, HEAD)),
                whole((HEAD + TAIL, HEAD)),
            ],
            scratch_shapes=[
                pltpu.VMEM((features, HEAD), BF16),
                pltpu.VMEM((features, HEAD), BF16),
                pltpu.VMEM((8, length), F32),
                pltpu.VMEM((8, length), F32),
            ],
        ),
        out_shape=[
            jax.ShapeDtypeStruct((length, HEAD), BF16),
            jax.ShapeDtypeStruct((length, HEAD), BF16),
            jax.ShapeDtypeStruct((8, length), F32),
            state_shape,
            state_shape,
        ],
        compiler_params=params(),
        cost_estimate=pl.CostEstimate(flops=6 * length * features * HEAD, transcendentals=0, bytes_accessed=8 << 20),
        name="keys",
    )(tab, *parts, *key_pieces, *value_pieces, gate_rows, bias, extra)

    if ringed:
        before = [along(state_f, hop) for hop in range(1, quarters)]
        after = [along(state_b, -hop) for hop in range(1, quarters)]
    else:
        before, after = far_states(state_f, state_b, quarter, quarters, lines)

    glu, glu_head, glu_tail = pl.pallas_call(
        functools.partial(glu_kernel, (group, blocks, rows, n_parts, n_pieces)),
        grid_spec=pltpu.PrefetchScalarGridSpec(
            num_scalar_prefetch=1,
            grid=(group,),
            in_specs=part_specs() + piece_specs(channels) * 2,
            out_specs=[
                pl.BlockSpec((count, channels), lambda i, tab: (i, 0)),
                whole((HALO, channels)),
                whole((HALO, channels)),
            ],
            scratch_shapes=[pltpu.VMEM((features, channels), BF16)] * 2,
        ),
        out_shape=[
            jax.ShapeDtypeStruct((length, channels), BF16),
            jax.ShapeDtypeStruct((HALO, channels), BF16),
            jax.ShapeDtypeStruct((HALO, channels), BF16),
        ],
        compiler_params=params(),
        cost_estimate=pl.CostEstimate(flops=4 * length * features * channels, transcendentals=0, bytes_accessed=8 << 20),
        name="glu",
    )(tab, *parts, *glu_pieces, *gate_pieces)

    glu_before = along(glu_tail, 1)
    glu_after = along(glu_head, -1)
    taps = lax.dynamic_slice_in_dim(conv_taps, place * channels, channels, 1)
    conv, stats = pl.pallas_call(
        conv_kernel,
        out_shape=[
            jax.ShapeDtypeStruct((length, channels), F32),
            jax.ShapeDtypeStruct((8, length), F32),
        ],
        scratch_shapes=[pltpu.VMEM((length + 2 * HALO, channels), F32)],
        compiler_params=params(),
        cost_estimate=pl.CostEstimate(flops=4 * length * features * channels, transcendentals=0, bytes_accessed=2 << 20),
        name="conv",
    )(glu, glu_before, glu_after, taps)
    stats = stats + swap(stats) if paired else lax.psum(stats, "tp")
    all_stats = [in_plane(stats, slot) for slot in slots]
    own_ln_gain = lax.dynamic_slice_in_dim(ln_gain, place * channels, channels, 0)[None, :]
    own_ln_bias = lax.dynamic_slice_in_dim(ln_bias, place * channels, channels, 0)[None, :]
    acts = pl.pallas_call(
        functools.partial(act_kernel, (group, conv_all)),
        grid_spec=pltpu.PrefetchScalarGridSpec(
            num_scalar_prefetch=1,
            grid=(1,),
            in_specs=[whole((length, channels))] + [whole((8, length))] * group + [whole((1, channels))] * 2,
            out_specs=[whole((count, channels))] * group,
        ),
        out_shape=[jax.ShapeDtypeStruct((count, channels), BF16)] * group,
        compiler_params=params(),
        cost_estimate=pl.CostEstimate(flops=2 * length * features * channels, transcendentals=0, bytes_accessed=2 << 20),
        name="act",
    )(tab, conv, *all_stats, own_ln_gain, own_ln_bias)
    acts = [in_plane(act, slot) for slot, act in enumerate(acts)]

    own_mem_gain = lax.dynamic_slice_in_dim(mem_gain, place * HEAD, HEAD, 0)[None, :]
    memories = pl.pallas_call(
        functools.partial(
            memory_kernel, (group, blocks, rows, n_parts, n_pieces, len(before), quarters, key_scale)
        ),
        grid_spec=pltpu.PrefetchScalarGridSpec(
            num_scalar_prefetch=1,
            grid=(group,),
            in_specs=part_specs()
            + piece_specs(HEAD)
            + [
                whole((length, HEAD)),
                whole((length, HEAD)),
                whole((8, length)),
                pl.BlockSpec((8, count), lambda i, tab: (0, i)),
                pl.BlockSpec((count, HEAD), lambda i, tab: (i, 0)),
                pl.BlockSpec((count, HEAD), lambda i, tab: (i, 0)),
            ]
            + [whole((HEAD + TAIL, HEAD))] * (2 * len(before))
            + [whole((1, HEAD))],
            out_specs=[whole((count, HEAD))] * group,
            scratch_shapes=[
                pltpu.VMEM((features, HEAD), BF16),
                pltpu.VMEM((2, HEAD, HEAD), BF16),
                pltpu.VMEM((2, HEAD, HEAD), BF16),
                pltpu.VMEM((8, HEAD), F32),
            ],
        ),
        out_shape=[jax.ShapeDtypeStruct((count, HEAD), BF16)] * group,
        compiler_params=params(),
        cost_estimate=pl.CostEstimate(flops=4 * length * features * HEAD, transcendentals=0, bytes_accessed=8 << 20),
        name="memory",
    )(tab, *parts, *query_pieces, keys, values, table, table, keys, values, *before, *after, own_mem_gain)
    memories = [in_plane(memory, slot) for slot, memory in enumerate(memories)]

    width = out_conv.shape[1]
    tile = 512
    halves = 2 if paired else 1
    partial = pl.pallas_call(
        functools.partial(out_kernel, (group, halves)),
        grid_spec=pltpu.PrefetchScalarGridSpec(
            num_scalar_prefetch=1,
            grid=(width // tile,),
            in_specs=[whole((count, channels))] * group
            + [whole((count, HEAD))] * group
            + [
                pl.BlockSpec((group * channels, tile), lambda i, tab: (0, i)),
                pl.BlockSpec((group * HEAD, tile), lambda i, tab: (0, i)),
            ],
            out_specs=[pl.BlockSpec((count // halves, tile), lambda i, tab: (0, i))] * halves,
            scratch_shapes=[pltpu.VMEM((count, tile), F32)],
        ),
        out_shape=[jax.ShapeDtypeStruct((count // halves, width), BF16)] * halves,
        compiler_params=params(),
        cost_estimate=pl.CostEstimate(
            flops=4 * count * width * group * HEAD, transcendentals=0, bytes_accessed=10 << 20
        ),
        name="out",
    )(out_tab, *acts, *memories, out_conv, out_mem)
    if paired:
        return (partial[0].astype(F32) + swap(partial[1]).astype(F32)).astype(BF16)
    return lax.psum_scatter(partial[0], "tp", scatter_dimension=0, tiled=True)


def far_states(state_f, state_b, quarter, quarters, lines):
    found = []
    for state, reverse in ((state_f, False), (state_b, True)):
        pieces = lax.all_gather(state, "sp", axis_index_groups=lines).astype(F32)
        if reverse:
            pieces = jnp.flip(pieces, 0)
        at = quarters - 1 - quarter if reverse else quarter
        totals = pieces[:, HEAD + 3, 0] + pieces[:, HEAD + 4, 0] + pieces[:, HEAD + 5, 0]
        levels = pieces[:, HEAD + 6, 0] + pieces[:, HEAD + 7, 0] + pieces[:, HEAD + 8, 0]
        order = jnp.arange(quarters)
        between = (order[None, :] > order[:, None]) & (order[None, :] < at)
        levels = levels + jnp.sum(jnp.where(between, totals[None, :], 0.0), axis=1)
        levels = jnp.where(order < at, levels, LOW_START)
        best = jnp.max(levels)
        weights = jnp.exp(levels - best)
        mat = jnp.sum(weights[:, None, None] * pieces[:, :HEAD], axis=0)
        vec = jnp.sum(weights[:, None] * (pieces[:, HEAD] + pieces[:, HEAD + 1] + pieces[:, HEAD + 2]), axis=0)
        found.append([compose_line(jnp.zeros((), F32), best, mat, vec)])
    return found


def solution(mesh):
    in_specs = (
        P("sp", "tp"),
        P(),
        P("sp", "tp"),
        P("sp", "tp"),
        P(None, "tp"),
        P("tp"),
        P("tp"),
        P("sp", "tp"),
        P("sp", "tp"),
        P("sp", "tp"),
        P(),
        P(),
        P("sp", None),
        P("tp"),
        P("tp", None),
        P("tp", None),
    )
    out_specs = P(("sp", "tp"), None)
    return jax.shard_map(shards, mesh=mesh, in_specs=in_specs, out_specs=out_specs, check_vma=False)
```

```python
import functools
import jax
import jax.numpy as jnp
from jax import lax
from jax.experimental import pallas as pl
from jax.experimental.pallas import tpu as pltpu
from jax.sharding import PartitionSpec as P


MEMORY_HEADS = 8
HEAD = 256
KW = 31
REACH = KW // 2
HALO = 16
TAIL = 16

EPS = 1e-06
LOW_START = -1e30
RING_MOST = 8
F32 = jnp.float32
BF16 = jnp.bfloat16


def params(**kw):
    return pltpu.CompilerParams(vmem_limit_bytes=24 * 1024 * 1024, **kw)


def whole(shape):
    return pl.BlockSpec(shape, lambda i, tab: (0,) * len(shape))


def dot(a, b):
    return jnp.dot(a, b, preferred_element_type=F32)


def dot_nt(a, b, **kw):
    return lax.dot_general(a, b, (((1,), (1,)), ((), ())), preferred_element_type=F32, **kw)


def dot_tn(a, b):
    return lax.dot_general(a, b, (((0,), (0,)), ((), ())), preferred_element_type=F32)


def scan_lanes(x, op, identity, reverse):
    width = x.shape[1]
    lane = lax.broadcasted_iota(jnp.int32, x.shape, 1)
    step = 1
    while step < width:
        if reverse:
            moved = pltpu.roll(x, width - step, 1)
            keep = lane < width - step
        else:
            moved = pltpu.roll(x, step, 1)
            keep = lane >= step
        x = op(x, jnp.where(keep, moved, identity))
        step *= 2
    return x


def log_sigmoid(x):
    return jnp.minimum(x, 0.0) - jnp.log1p(jnp.exp(-jnp.abs(x)))


def split3(x):
    high = x.astype(BF16)
    rest = x - high.astype(F32)
    mid = rest.astype(BF16)
    low = (rest - mid.astype(F32)).astype(BF16)
    return high.astype(F32), mid.astype(F32), low.astype(F32)


def fetch(copies):
    made = [pltpu.make_async_copy(source, target, sem) for source, target, sem in copies]
    for copy in made:
        copy.start()
    return made


def fetch_parts(tab, group, parts, held, sems):
    count, wide = held.shape[2:]
    copies = []
    for block in range(group):
        rows = pl.ds(pl.multiple_of(tab[2 * group + block] * count, count), count)
        for place, part in enumerate(parts):
            copies.append(
                (part.at[rows, pl.ds(0, wide)], held.at[place, block], sems.at[block * len(parts) + place])
            )
    made = fetch(copies)
    return [made[block * len(parts) : (block + 1) * len(parts)] for block in range(group)]


def fetch_weights(tab, group, blocks, rows, pieces, scratches, sems):
    kinds = len(scratches)
    first = 3 * group + 5
    per = pieces[0].shape[0] // (rows * kinds)
    copies = []
    for block in range(blocks):
        start = pl.multiple_of(tab[first + block], rows)
        for kind, scratch in enumerate(scratches):
            at = (block % per * kinds + kind) * rows
            copies.append(
                (pieces[block // per].at[pl.ds(at, rows), :], scratch.at[pl.ds(start, rows), :], sems.at[kind])
            )
    fetch(copies)
    return [pltpu.make_async_copy(x, x, sems.at[kind]) for kind, x in enumerate(scratches)]


def arrived(copies):
    for copy in copies:
        copy.wait()


def project(held, weights):
    total = None
    for place, part in enumerate(held):
        wide = part.shape[1]
        term = dot(part, weights[place * wide : (place + 1) * wide, :])
        total = term if total is None else total + term
    return total


def gates_kernel(dims, tab, *refs):
    group, n_parts, extra_at, key_scale = dims
    parts = refs[:n_parts]
    extra, gate_rows, gate_bias, rows_out, held, extra_in, rows_in, gates, extras, part_sems, sems = refs[n_parts:]
    core, head = tab[3 * group + 2], tab[3 * group + 4]
    waits = fetch_parts(tab, group, parts, held, part_sems)
    count = held.shape[2]
    copies = [(gate_rows, rows_in, sems.at[group])]
    for block in range(group):
        rows = pl.ds(pl.multiple_of(tab[2 * group + block] * count, count), count)
        copies.append((extra.at[rows, pl.ds(extra_at * 128, 128)], extra_in.at[block], sems.at[block]))
    rows_wait, *extra_waits = fetch(copies)
    line = lax.broadcasted_iota(jnp.int32, (2 * MEMORY_HEADS, 128), 0)
    column = lax.broadcasted_iota(jnp.int32, (2 * MEMORY_HEADS, 128), 1)
    select = (column % (2 * MEMORY_HEADS) == line) & (column < 6 * MEMORY_HEADS)
    select = jnp.where(select, 1.0, 0.0).astype(BF16)
    rows_wait.wait()
    for block in range(group):
        here = slice(block * count, (block + 1) * count)
        arrived(waits[block])
        pre = None
        for place in range(n_parts):
            wide = held.shape[3]
            start = 0 if n_parts == 1 else pl.multiple_of((core if place == 0 else 1 - core) * wide, wide)
            term = dot_nt(rows_in[:, pl.ds(start, wide)], held[place, block])
            pre = term if pre is None else pre + term
        gates[:, here] = pre
        extra_waits[block].wait()
        extras[:, here] = dot_nt(select, extra_in[block])
    width = gates.shape[1]

    def gate(kind):
        return gates[pl.ds(kind * MEMORY_HEADS + head, 1), :] + gate_bias[kind * MEMORY_HEADS + head]

    sub = lax.broadcasted_iota(jnp.int32, (8, width), 0)
    forget_f = log_sigmoid(gate(1)) + extras[pl.ds(head, 1), :]
    forget_b = log_sigmoid(gate(3)) + extras[pl.ds(MEMORY_HEADS + head, 1), :]
    decay_f = scan_lanes(jnp.broadcast_to(forget_f, (8, width)), jnp.add, 0.0, False)[0:1]
    decay_b = scan_lanes(jnp.broadcast_to(forget_b, (8, width)), jnp.add, 0.0, True)[0:1]
    level_f, level_b = gate(0) - decay_f, gate(2) - decay_b
    peak_f = scan_lanes(jnp.broadcast_to(level_f, (8, width)), jnp.maximum, LOW_START, False)[0:1]
    peak_b = scan_lanes(jnp.broadcast_to(level_b, (8, width)), jnp.maximum, LOW_START, True)[0:1]
    most_f = jnp.max(level_f, axis=1, keepdims=True)
    most_b = jnp.max(level_b, axis=1, keepdims=True)
    end_f, end_b = jnp.exp(level_f - most_f) * key_scale, jnp.exp(level_b - most_b) * key_scale
    vectors = [level_f, level_b, decay_f, decay_b, peak_f, peak_b, end_f, end_b]
    table = jnp.zeros((8, width), F32)
    for place, vector in enumerate(vectors):
        table = jnp.where(sub == place, vector, table)
    rows_out[...] = table


def front_kernel(dims, tab, *refs):
    group, blocks, rows, n_parts, n_pieces = dims
    parts, pieces = refs[:n_parts], refs[n_parts : n_parts + n_pieces]
    glu_out, head_out, tail_out, held, value_w, gate_w, part_sems, sems = refs[n_parts + n_pieces :]
    weight_waits = fetch_weights(tab, group, blocks, rows, pieces, (value_w, gate_w), sems)
    waits = fetch_parts(tab, group, parts, held, part_sems)
    arrived(weight_waits)
    count = held.shape[2]
    for block in range(group):
        arrived(waits[block])
        have = [held[place, block] for place in range(n_parts)]
        glu = (project(have, value_w) * jax.nn.sigmoid(project(have, gate_w))).astype(BF16)
        glu_out[block * count : (block + 1) * count, :] = glu
        if block == 0:
            head_out[...] = glu[0:HALO, :]
        if block == group - 1:
            tail_out[...] = glu[count - HALO :, :]


def states_kernel(dims, tab, *refs):
    group, blocks, rows, n_parts, n_pieces, quarters, n_sends = dims
    refs = list(refs)
    parts = [refs.pop(0) for _ in range(n_parts)]
    key_pieces = [refs.pop(0) for _ in range(n_pieces)]
    value_pieces = [refs.pop(0) for _ in range(n_pieces)]
    table_in, key_out, value_out = [refs.pop(0) for _ in range(3)]
    sends = [refs.pop(0) for _ in range(n_sends)]
    held, key_w, value_w, table, part_sems, sems = refs
    key_wait = fetch_weights(tab, group, blocks, rows, key_pieces, (key_w,), sems.at[pl.ds(0, 1)])
    value_wait = fetch_weights(tab, group, blocks, rows, value_pieces, (value_w,), sems.at[pl.ds(1, 1)])
    table_wait = fetch([(table_in, table, sems.at[2])])
    waits = fetch_parts(tab, group, parts, held, part_sems)
    arrived(key_wait)
    arrived(value_wait)
    arrived(table_wait)
    count = held.shape[2]
    columns = jnp.transpose(table[...])
    mats, sums = [None, None], [None, None]
    for block in range(group):
        here = slice(block * count, (block + 1) * count)
        arrived(waits[block])
        have = [held[place, block] for place in range(n_parts)]
        keys = project(have, key_w).astype(BF16)
        key_out[here, :] = keys
        values = project(have, value_w).astype(BF16)
        value_out[here, :] = values
        keys = keys.astype(F32)
        for place in range(2):
            weighted = keys * columns[here, 6 + place : 7 + place]
            line = jnp.sum(weighted, axis=0, keepdims=True)
            mat = dot_tn(weighted.astype(BF16), values)
            sums[place] = line if block == 0 else sums[place] + line
            mats[place] = mat if block == 0 else mats[place] + mat
    width = table.shape[1]
    at = lax.broadcasted_iota(jnp.int32, (TAIL, HEAD), 0)
    made = []
    for place, lane in ((0, width - 1), (1, 0)):
        total = table[2 + place : 3 + place, lane : lane + 1]
        most = table[4 + place : 5 + place, lane : lane + 1]
        lines = (*split3(sums[place]), *split3(total), *split3(total + most))
        tail = jnp.zeros((TAIL, HEAD), F32)
        for line, value in enumerate(lines):
            tail = jnp.where(at == line, value, tail)
        made.append((mats[place].astype(BF16), tail.astype(BF16)))
    for slot, send in enumerate(sends):
        if n_sends == quarters - 1 and quarters > 1:
            ahead = tab[3 * group] + slot + 1 < quarters
            for chosen, (mat, tail) in ((ahead, made[0]), (jnp.logical_not(ahead), made[1])):

                @pl.when(chosen)
                def _(mat=mat, tail=tail, send=send):
                    send[0:HEAD, :] = mat
                    send[HEAD:, :] = tail
        else:
            send[0:HEAD, :] = made[slot][0]
            send[HEAD:, :] = made[slot][1]


def local_kernel(dims, tab, *refs):
    group, blocks, rows, n_parts, n_pieces, key_scale = dims
    parts, pieces = refs[:n_parts], refs[n_parts : n_parts + n_pieces]
    keys_in, values_in, table_in = refs[n_parts + n_pieces : n_parts + n_pieces + 3]
    query_out, numer_f, numer_b, denom_out = refs[n_parts + n_pieces + 3 : n_parts + n_pieces + 7]
    held, query_w, keys, values, table, part_sems, sems = refs[n_parts + n_pieces + 7 :]
    weight_wait = fetch_weights(tab, group, blocks, rows, pieces, (query_w,), sems.at[pl.ds(3, 1)])
    waits = fetch_parts(tab, group, parts, held, part_sems)
    others_wait = fetch(
        [(keys_in, keys, sems.at[0]), (values_in, values, sems.at[1]), (table_in, table, sems.at[2])]
    )
    arrived(weight_wait)
    length = keys.shape[0]
    count = length // group
    spot_t = lax.broadcasted_iota(jnp.int32, (count, count), 0)
    spot_s = lax.broadcasted_iota(jnp.int32, (count, count), 1)
    masks = (spot_s <= spot_t, spot_s >= spot_t)
    lane = lax.broadcasted_iota(jnp.int32, (count, 128), 1)
    for block in range(group):
        here = slice(block * count, (block + 1) * count)
        arrived(waits[block])
        queries = project([held[place, block] for place in range(n_parts)], query_w).astype(BF16)
        query_out[here, :] = queries
        if block == 0:
            arrived(others_wait)
        raw = dot_nt(queries, keys[...]) * key_scale
        columns = jnp.transpose(table[:, here])
        denoms = []
        for way, out in enumerate((numer_f, numer_b)):
            top = columns[:, 4 + way : 5 + way]
            power = jnp.where(masks[way], table[way : way + 1, here] - top, LOW_START)
            scores = raw[:, here] * jnp.exp(power)
            denom = jnp.sum(scores, axis=1, keepdims=True)
            numer = dot(scores.astype(BF16), values[here, :])
            others = slice(0, block * count) if way == 0 else slice((block + 1) * count, length)
            if others.stop > others.start:
                scores = raw[:, others] * jnp.exp(table[way : way + 1, others] - top)
                denom = denom + jnp.sum(scores, axis=1, keepdims=True)
                numer = numer + dot(scores.astype(BF16), values[others, :])
            out[here, :] = numer.astype(BF16)
            denoms.append(denom)
        denom_out[here, :] = jnp.where(lane == 0, denoms[0], denoms[1])


def conv_kernel(tab, glu, before, after, taps, conv_out, stats_out, padded, sums):
    length, width = glu.shape
    padded[0:HALO, :] = before[...].astype(F32)
    padded[HALO : HALO + length, :] = glu[...].astype(F32)
    padded[HALO + length :, :] = after[...].astype(F32)
    chunk = 64
    lead = HALO - REACH
    lane = lax.broadcasted_iota(jnp.int32, (chunk, 128), 1)

    def one(step, carry):
        base = pl.multiple_of(step * chunk, chunk)
        line = jnp.zeros((chunk, 128), F32)
        square = jnp.zeros((chunk, 128), F32)
        for left in range(0, width, 128):
            lanes = slice(left, left + 128)
            total = jnp.zeros((chunk, 128), F32)
            window_all = padded[pl.ds(base, chunk + 32), lanes]
            for shift in range(8):
                window = pltpu.roll(window_all, chunk + 32 - shift, 0) if shift else window_all
                for high in range(4):
                    tap = 8 * high + shift - lead
                    if 0 <= tap < KW:
                        total = total + taps[tap : tap + 1, lanes] * window[8 * high : 8 * high + chunk, :]
            conv_out[pl.ds(base, chunk), lanes] = total
            line = line + total
            square = square + total * total
        line = jnp.sum(line, axis=1, keepdims=True)
        square = jnp.sum(square, axis=1, keepdims=True)
        sums[pl.ds(base, chunk), :] = jnp.where(lane == 0, line, square)
        return carry

    lax.fori_loop(0, length // chunk, one, 0)
    stats_out[...] = jnp.transpose(sums[...])[0:8, :]


def act_kernel(dims, tab, conv, *refs):
    group, channels, halves = dims
    stats, (gain, bias), outs = refs[:group], refs[group : group + 2], refs[group + 2 :]
    total = stats[0][...]
    for more in stats[1:]:
        total = total + more[...]
    mean = total[0:1, :] / channels
    var = total[1:2, :] / channels - mean * mean
    scale = lax.rsqrt(var + EPS)
    sub = lax.broadcasted_iota(jnp.int32, total.shape, 0)
    columns = jnp.transpose(jnp.where(sub == 0, mean, scale))
    count = outs[0].shape[0]
    for slot, out in enumerate(outs):
        which = tab[group + slot]
        start = pl.multiple_of(which * count, count)
        picked = columns[0:count, :]
        for block in range(1, group):
            picked = jnp.where(which == block, columns[block * count : (block + 1) * count, :], picked)
        normal = (conv[pl.ds(start, count), :] - picked[:, 0:1]) * picked[:, 1:2]
        normal = normal * gain[...] + bias[...]
        place_rows(tab, group, halves, out, (normal * jax.nn.sigmoid(normal)).astype(BF16))


def place_rows(tab, group, halves, out, value):
    if halves == 1:
        out[...] = value
        return
    half = value.shape[0] // 2
    own = tab[3 * group + 2]
    out[pl.ds(pl.multiple_of((1 - own) * half, half), half), :] = value[:half, :]
    out[pl.ds(pl.multiple_of(own * half, half), half), :] = value[half:, :]


def incoming(pieces):
    levels, best, passed = [], jnp.full((1, HEAD), LOW_START, F32), jnp.zeros((1, HEAD), F32)
    for piece, there in pieces:
        lines = piece[HEAD:, :].astype(F32)
        level = lines[6:7] + lines[7:8] + lines[8:9] + passed
        if there is not None:
            level = jnp.where(there, level, LOW_START)
        levels.append(level)
        best = jnp.maximum(best, level)
        passed = passed + lines[3:4] + lines[4:5] + lines[5:6]
    mat, vec = jnp.zeros((HEAD, HEAD), F32), jnp.zeros((1, HEAD), F32)
    for (piece, there), level in zip(pieces, levels):
        weight = jnp.exp(level - best)
        if there is not None:
            weight = jnp.where(there, weight, 0.0)
        lines = piece[HEAD:, :].astype(F32)
        mat = mat + weight * piece[0:HEAD, :].astype(F32)
        vec = vec + weight * (lines[0:1] + lines[1:2] + lines[2:3])
    return mat, vec, best


def finish_kernel(dims, tab, *refs):
    group, n_states, ringed, halves = dims
    queries_in, numer_f, numer_b, denoms_in, table_in = refs[:5]
    states_in, gain = refs[5 : 5 + n_states], refs[5 + n_states]
    outs = refs[6 + n_states : 6 + n_states + group]
    states, table, queries_all, numers, denoms_all, result, sems, block_sems = refs[6 + n_states + group :]
    length = queries_in.shape[0]
    count = length // group
    first = fetch(
        [(state, states.at[slot], sems.at[slot]) for slot, state in enumerate(states_in)]
        + [(table_in, table, sems.at[n_states])]
    )
    waits = []
    for block in range(group):
        here = pl.ds(block * count, count)
        waits.append(
            fetch(
                [
                    (queries_in.at[here, :], queries_all.at[here, :], block_sems.at[block, 0]),
                    (numer_f.at[here, :], numers.at[0, here, :], block_sems.at[block, 1]),
                    (numer_b.at[here, :], numers.at[1, here, :], block_sems.at[block, 2]),
                    (denoms_in.at[here, :], denoms_all.at[here, :], block_sems.at[block, 3]),
                ]
            )
        )
    arrived(first)
    pieces = [states.at[slot] for slot in range(n_states)]
    if ringed:
        at = tab[3 * group]
        ahead = [(state, slot + 1 <= at) for slot, state in enumerate(pieces)]
        back = [(state, slot + 1 > at) for slot, state in enumerate(pieces)][::-1]
    else:
        ahead, back = [(pieces[0], None)], [(pieces[1], None)]
    mats, vecs, bests = [], [], []
    for these in (ahead, back):
        mat, vec, best = incoming(these)
        high = mat.astype(BF16)
        mats.append((high, (mat - high.astype(F32)).astype(BF16)))
        vecs.append(vec)
        bests.append(best[:, 0:1])
    line = lax.broadcasted_iota(jnp.int32, (128, HEAD), 0)
    vec = jnp.where(line == 0, vecs[0], vecs[1])
    vec_high = vec.astype(BF16)
    vec_low = (vec - vec_high.astype(F32)).astype(BF16)
    sub = lax.broadcasted_iota(jnp.int32, (8, length), 0)
    peak = jnp.where(sub == 0, table[4:5, :], table[5:6, :])
    decay = jnp.where(sub == 0, table[2:3, :], table[3:4, :])
    best = jnp.where(sub == 0, bests[0], bests[1])
    top = jnp.maximum(peak, best)
    carry = jnp.transpose(jnp.exp(best - top))
    stay = jnp.transpose(jnp.exp(peak - top))
    floor = jnp.transpose(jnp.exp(-(decay + top)))
    for block in range(group):
        here = slice(block * count, (block + 1) * count)
        arrived(waits[block])
        queries = queries_all[here, :]
        along = (dot_nt(queries, vec_high) + dot_nt(queries, vec_low))[:, 0:8]
        denom = stay[here, :] * denoms_all[here, 0:8] + carry[here, :] * along
        inverse = 1.0 / jnp.maximum(jnp.abs(denom), floor[here, :])
        left, right = stay[here, :] * inverse, carry[here, :] * inverse
        summed = None
        for way, (high, low) in enumerate(mats):
            term = left[:, way : way + 1] * numers[way, here, :].astype(F32)
            term = term + right[:, way : way + 1] * (dot(queries, high) + dot(queries, low))
            summed = term if summed is None else summed + term
        scale = lax.rsqrt(jnp.mean(summed * summed, axis=1, keepdims=True) + EPS)
        result[here, :] = (summed * scale * gain[...]).astype(BF16)
    for slot, out in enumerate(outs):
        start = pl.multiple_of(tab[group + slot] * count, count)
        place_rows(tab, group, halves, out, result[pl.ds(start, count), :])


def compose_line(total, level, mat, vec):
    tail = jnp.concatenate([jnp.broadcast_to(x[None, :], (1, HEAD)) for x in (*split3(vec), *split3(total + jnp.zeros((HEAD,), F32)), *split3(level + jnp.zeros((HEAD,), F32)))])
    tail = jnp.concatenate([tail, jnp.zeros((TAIL - tail.shape[0], HEAD), F32)])
    return jnp.concatenate([mat, tail]).astype(BF16)


def shards(
    tokens,
    norm_gain,
    glu_value,
    glu_gate,
    conv_taps,
    ln_gain,
    ln_bias,
    query_weight,
    key_weight,
    value_weight,
    gate_weight,
    gate_bias,
    log_decay_extra,
    mem_gain,
    out_conv,
    out_mem,
):
    sp, tp = lax.axis_size("sp"), lax.axis_size("tp")
    group = mem_gain.shape[0] // HEAD
    quarters = sp // group
    count = tokens.shape[0]
    length = group * count
    rows = key_weight.shape[0]
    features = norm_gain.shape[0]
    channels = conv_taps.shape[1] // group
    conv_all = channels * group * tp
    blocks = sp
    key_scale = HEAD ** (-0.5)
    me, core = lax.axis_index("sp"), lax.axis_index("tp")
    place, quarter = me % group, me // group
    paired = tp == 2
    even = group & (group - 1) == 0
    ringed = quarters <= RING_MOST

    def source(p, slot):
        return p ^ slot if even else (p - slot) % group

    def target(p, slot):
        return p ^ slot if even else (p + slot) % group

    def in_plane(x, slot):
        if slot == 0:
            return x
        pairs = [(i, i - i % group + target(i % group, slot)) for i in range(sp)]
        return lax.ppermute(x, "sp", pairs)

    def along(x, hops, ring=False):
        pairs = [(i, i + hops * group) for i in range(sp)]
        pairs = [(i, j % sp) for i, j in pairs] if ring else [(i, j) for i, j in pairs if 0 <= j < sp]
        return lax.ppermute(x, "sp", pairs)

    def swap(x):
        return lax.ppermute(x, "tp", [(0, 1), (1, 0)])

    lines = [[k * group + j for k in range(quarters)] for j in range(group)]

    def tall(x):
        return jnp.concatenate(x, axis=0) if len(x) > 1 else x[0]

    def split_weights(weights, width):
        got = []
        for slot in range(group):
            to = target(place, slot) * width
            sent = tall([lax.dynamic_slice_in_dim(weight, to, width, 1) for weight in weights])
            got.append(in_plane(sent, slot))
        return got

    def ring(piece):
        if not ringed:
            return [lax.all_gather(piece, "sp", axis=0, tiled=True, axis_index_groups=lines)]
        pieces = [piece]
        for _ in range(1, quarters):
            pieces.append(along(pieces[-1], 1, True))
        return pieces

    slots = list(range(group))
    sources = [source(place, slot) for slot in slots]
    targets = [target(place, slot) for slot in slots]
    inverse = [p ^ place if even else (place - p) % group for p in slots]
    shift = core * tokens.shape[1] if paired else 0
    offsets = []
    for hop in range(quarters):
        block_quarter = (quarter - hop) % quarters if ringed else hop
        for slot in slots:
            offsets.append(((block_quarter * group + sources[slot]) * rows - shift) % features)
    head = core * group + place
    entries = (*sources, *targets, *inverse, quarter, 0, core, place, head, *offsets)
    tab = jnp.stack([jnp.asarray(x, jnp.int32) for x in entries])

    got = split_weights([glu_value, glu_gate, key_weight], channels)
    glu_piece = tall([x[: 2 * rows] for x in got])
    key_piece = tall([x[2 * rows :] for x in got])
    wide = tokens.astype(F32)
    squares = jnp.sum(wide * wide, axis=-1, keepdims=True)
    squares = squares + swap(squares) if paired else lax.psum(squares, "tp")
    own_gain = lax.dynamic_slice_in_dim(norm_gain, core * tokens.shape[1], tokens.shape[1], 0)
    normed = (wide * lax.rsqrt(squares / features + EPS) * own_gain).astype(BF16)
    extras = [part.astype(BF16) for part in split3(log_decay_extra)]
    extras = jnp.pad(jnp.concatenate(extras, 1), ((0, 0), (0, 128 - 3 * 2 * MEMORY_HEADS)))
    own_width = tokens.shape[1]
    payload = jnp.concatenate([normed, extras], 1)
    payload = tall([in_plane(payload, slot) for slot in slots])
    if paired:
        parts, extra_at = [payload, swap(payload)], own_width // 128
        extra = payload
        part_width = own_width
    else:
        parts, extra_at = [lax.all_gather(payload[:, :own_width], "tp", axis=1, tiled=True)], 0
        extra = payload[:, own_width:]
        part_width = features
    glu_pieces = ring(glu_piece)
    got = split_weights([value_weight, query_weight], HEAD)
    value_piece, query_piece = [tall([x[m * rows : (m + 1) * rows] for x in got]) for m in range(2)]
    conv_rows = tall([lax.dynamic_slice_in_dim(out_conv, at * channels, channels, 0) for at in sources])
    mem_rows = tall([lax.dynamic_slice_in_dim(out_mem, at * HEAD, HEAD, 0) for at in sources])
    key_pieces = ring(key_piece)
    value_pieces = ring(value_piece)
    query_pieces = ring(query_piece)

    def far(arrays):
        return [pl.BlockSpec(memory_space=pl.ANY) for _ in arrays]

    def wholes(shapes):
        return [whole(x.shape) for x in shapes]

    def dma(*dims):
        return pltpu.SemaphoreType.DMA(dims)

    def call(kernel, in_specs, out_specs, out_shape, scratch, flops, steps=1):
        return pl.pallas_call(
            kernel,
            grid_spec=pltpu.PrefetchScalarGridSpec(
                num_scalar_prefetch=1,
                grid=(steps,),
                in_specs=in_specs,
                out_specs=out_specs,
                scratch_shapes=scratch,
            ),
            out_shape=out_shape,
            compiler_params=params(),
            cost_estimate=pl.CostEstimate(flops=flops, transcendentals=0, bytes_accessed=4 << 20),
        )

    def shape(dims, kind=BF16):
        return jax.ShapeDtypeStruct(dims, kind)

    n_parts, n_pieces = len(parts), len(key_pieces)
    halves = 2 if paired else 1
    work = 2 * length * features * HEAD
    held = [pltpu.VMEM((n_parts, group, count, part_width), BF16)]
    part_sems = [dma(group * n_parts)]
    square = [pltpu.VMEM((features, HEAD), BF16)]
    table = call(
        functools.partial(gates_kernel, (group, n_parts, extra_at, key_scale)),
        far(parts) + far([extra, gate_weight]) + [pl.BlockSpec(memory_space=pltpu.SMEM)],
        whole((8, length)),
        shape((8, length), F32),
        held
        + [pltpu.VMEM((group, count, 128), BF16), pltpu.VMEM((4 * MEMORY_HEADS, features), BF16)]
        + [pltpu.VMEM((4 * MEMORY_HEADS, length), F32), pltpu.VMEM((2 * MEMORY_HEADS, length), F32)]
        + part_sems
        + [dma(group + 1)],
        work,
    )(tab, *parts, extra, gate_weight.T, gate_bias)

    made = [shape((length, channels)), shape((HALO, channels)), shape((HALO, channels))]
    glu, glu_head, glu_tail = call(
        functools.partial(front_kernel, (group, blocks, rows, n_parts, n_pieces)),
        far(parts) + far(glu_pieces),
        wholes(made),
        made,
        held + [pltpu.VMEM((features, channels), BF16)] * 2 + part_sems + [dma(2)],
        2 * work,
    )(tab, *parts, *glu_pieces)

    glu_before = along(glu_tail, 1)
    glu_after = along(glu_head, -1)

    def own_lanes(lines, width):
        return pl.BlockSpec((lines, width), lambda i, tab: (0, tab[3 * group + 3]))

    conv, stats = call(
        conv_kernel,
        [whole((length, channels)), whole((HALO, channels)), whole((HALO, channels)), own_lanes(KW, channels)],
        [whole((length, channels)), whole((8, length))],
        [shape((length, channels), F32), shape((8, length), F32)],
        [pltpu.VMEM((length + 2 * HALO, channels), F32), pltpu.VMEM((length, 128), F32)],
        2 * work,
        1,
    )(tab, glu, glu_before, glu_after, conv_taps)
    stats = stats + swap(stats) if paired else lax.psum(stats, "tp")
    all_stats = [in_plane(stats, slot) for slot in slots]
    acts = call(
        functools.partial(act_kernel, (group, conv_all, halves)),
        [whole((length, channels))] + [whole((8, length))] * group + [own_lanes(1, channels)] * 2,
        [whole((count, channels))] * group,
        [shape((count, channels))] * group,
        [],
        work,
        1,
    )(tab, conv, *all_stats, ln_gain[None, :], ln_bias[None, :])
    acts = [in_plane(act, slot) for slot, act in enumerate(acts)]

    n_sends = quarters - 1 if ringed else 2
    made = [shape((length, HEAD))] * 2 + [shape((HEAD + TAIL, HEAD))] * n_sends
    keys, values, *sends = call(
        functools.partial(states_kernel, (group, blocks, rows, n_parts, n_pieces, quarters, n_sends)),
        far(parts) + far(key_pieces) + far(value_pieces) + far([table]),
        wholes(made),
        made,
        held + square * 2 + [pltpu.VMEM((8, length), F32)] + part_sems + [dma(3)],
        2 * work,
    )(tab, *parts, *key_pieces, *value_pieces, table)
    if ringed:
        states = [along(send, hop + 1, True) for hop, send in enumerate(sends)]
    else:
        states = far_states(sends[0], sends[1], quarter, quarters, lines)

    tall_head = [pltpu.VMEM((length, HEAD), BF16)]
    made = [shape((length, HEAD))] * 3 + [shape((length, 128), F32)]
    locals_made = call(
        functools.partial(local_kernel, (group, blocks, rows, n_parts, n_pieces, key_scale)),
        far(parts) + far(query_pieces) + far([keys, values, table]),
        wholes(made),
        made,
        held + square + tall_head * 2 + [pltpu.VMEM((8, length), F32)] + part_sems + [dma(4)],
        work,
    )(tab, *parts, *query_pieces, keys, values, table)

    made = [shape((count, HEAD))] * group
    memories = call(
        functools.partial(finish_kernel, (group, len(states), ringed, halves)),
        far(locals_made) + far([table]) + far(states) + [own_lanes(1, HEAD)],
        wholes(made),
        made,
        [pltpu.VMEM((len(states), HEAD + TAIL, HEAD), BF16), pltpu.VMEM((8, length), F32)]
        + tall_head
        + [pltpu.VMEM((2, length, HEAD), BF16), pltpu.VMEM((length, 128), F32)]
        + tall_head
        + [dma(len(states) + 1), dma(group, 4)],
        work,
    )(tab, *locals_made, table, *states, mem_gain[None, :])
    memories = [in_plane(memory, slot) for slot, memory in enumerate(memories)]

    partial = dot(jnp.concatenate(acts, 1), conv_rows)
    result = (partial + dot(jnp.concatenate(memories, 1), mem_rows)).astype(BF16)
    if paired:
        half = count // 2
        return (result[half:].astype(F32) + swap(result[:half]).astype(F32)).astype(BF16)
    return lax.psum_scatter(result, "tp", scatter_dimension=0, tiled=True)


def far_states(state_f, state_b, quarter, quarters, lines):
    found = []
    for state, reverse in ((state_f, False), (state_b, True)):
        pieces = lax.all_gather(state, "sp", axis_index_groups=lines).astype(F32)
        if reverse:
            pieces = jnp.flip(pieces, 0)
        at = quarters - 1 - quarter if reverse else quarter
        totals = pieces[:, HEAD + 3, 0] + pieces[:, HEAD + 4, 0] + pieces[:, HEAD + 5, 0]
        levels = pieces[:, HEAD + 6, 0] + pieces[:, HEAD + 7, 0] + pieces[:, HEAD + 8, 0]
        order = jnp.arange(quarters)
        between = (order[None, :] > order[:, None]) & (order[None, :] < at)
        levels = levels + jnp.sum(jnp.where(between, totals[None, :], 0.0), axis=1)
        levels = jnp.where(order < at, levels, LOW_START)
        best = jnp.max(levels)
        weights = jnp.exp(levels - best)
        mat = jnp.sum(weights[:, None, None] * pieces[:, :HEAD], axis=0)
        vec = jnp.sum(weights[:, None] * (pieces[:, HEAD] + pieces[:, HEAD + 1] + pieces[:, HEAD + 2]), axis=0)
        found.append(compose_line(jnp.zeros((), F32), best, mat, vec))
    return found


def solution(mesh):
    in_specs = (
        P("sp", "tp"),
        P(),
        P("sp", "tp"),
        P("sp", "tp"),
        P(None, "tp"),
        P("tp"),
        P("tp"),
        P("sp", "tp"),
        P("sp", "tp"),
        P("sp", "tp"),
        P(),
        P(),
        P("sp", None),
        P("tp"),
        P("tp", None),
        P("tp", None),
    )
    out_specs = P(("sp", "tp"), None)

    return jax.shard_map(shards, mesh=mesh, in_specs=in_specs, out_specs=out_specs, check_vma=False)
```

```python
import functools
import jax
import jax.numpy as jnp
from jax import lax
from jax.experimental import pallas as pl
from jax.experimental.pallas import tpu as pltpu
from jax.sharding import PartitionSpec as P


MEMORY_HEADS = 8
HEAD = 256
KW = 31
REACH = KW // 2
HALO = 16
TAIL = 16

EPS = 1e-06
LOW_START = -1e30
RING_MOST = 8
F32 = jnp.float32
BF16 = jnp.bfloat16


def params(**kw):
    return pltpu.CompilerParams(vmem_limit_bytes=24 * 1024 * 1024, **kw)


def whole(shape):
    return pl.BlockSpec(shape, lambda i, tab: (0,) * len(shape))


def dot(a, b):
    return jnp.dot(a, b, preferred_element_type=F32)


def dot_nt(a, b, **kw):
    return lax.dot_general(a, b, (((1,), (1,)), ((), ())), preferred_element_type=F32, **kw)


def dot_tn(a, b):
    return lax.dot_general(a, b, (((0,), (0,)), ((), ())), preferred_element_type=F32)


def scan_lanes(x, op, identity, reverse):
    width = x.shape[1]
    lane = lax.broadcasted_iota(jnp.int32, x.shape, 1)
    step = 1
    while step < width:
        if reverse:
            moved = pltpu.roll(x, width - step, 1)
            keep = lane < width - step
        else:
            moved = pltpu.roll(x, step, 1)
            keep = lane >= step
        x = op(x, jnp.where(keep, moved, identity))
        step *= 2
    return x


def log_sigmoid(x):
    return jnp.minimum(x, 0.0) - jnp.log1p(jnp.exp(-jnp.abs(x)))


def split3(x):
    high = x.astype(BF16)
    rest = x - high.astype(F32)
    mid = rest.astype(BF16)
    low = (rest - mid.astype(F32)).astype(BF16)
    return high.astype(F32), mid.astype(F32), low.astype(F32)


def fetch(copies):
    made = [pltpu.make_async_copy(source, target, sem) for source, target, sem in copies]
    for copy in made:
        copy.start()
    return made


def fetch_parts(tab, parts, held, sems):
    group, wide = held.shape[1], held.shape[3]
    copies = []
    for spot, part in enumerate(parts):
        copies.append((part.at[:, pl.ds(0, wide)], held.at[spot // group, tab[spot % group]], sems.at[spot]))
    return fetch(copies)


def fetch_weights(tab, group, blocks, rows, pieces, scratches, sems, by_slot=False):
    kinds = len(scratches)
    first = 3 * group + 5
    per = pieces[0].shape[0] // (rows * kinds)
    copies = []
    for block in range(blocks):
        entry = block % per * group + block // per if by_slot else block
        start = pl.multiple_of(tab[first + entry], rows)
        for kind, scratch in enumerate(scratches):
            at = (block % per * kinds + kind) * rows
            copies.append(
                (pieces[block // per].at[pl.ds(at, rows), :], scratch.at[pl.ds(start, rows), :], sems.at[kind])
            )
    fetch(copies)
    return [pltpu.make_async_copy(x, x, sems.at[kind]) for kind, x in enumerate(scratches)]


def arrived(copies):
    for copy in copies:
        copy.wait()


def project(held, weights):
    total = None
    for place, part in enumerate(held):
        wide = part.shape[1]
        term = dot(part, weights[place * wide : (place + 1) * wide, :])
        total = term if total is None else total + term
    return total


def gates_kernel(dims, tab, *refs):
    group, n_parts, extra_at, key_scale = dims
    parts, extra = refs[:n_parts], refs[n_parts : n_parts + group]
    gate_rows, gate_bias, rows_out, held, extra_in, rows_in, gates, extras, part_sems, sems = refs[n_parts + group :]
    core, head = tab[3 * group + 2], tab[3 * group + 4]
    waits = fetch_parts(tab, parts, held, part_sems)
    count = held.shape[2]
    copies = [(gate_rows, rows_in, sems.at[group])]
    for slot, more in enumerate(extra):
        copies.append((more.at[:, pl.ds(extra_at * 128, 128)], extra_in.at[tab[slot]], sems.at[slot]))
    rows_wait, *extra_waits = fetch(copies)
    line = lax.broadcasted_iota(jnp.int32, (2 * MEMORY_HEADS, 128), 0)
    column = lax.broadcasted_iota(jnp.int32, (2 * MEMORY_HEADS, 128), 1)
    select = (column % (2 * MEMORY_HEADS) == line) & (column < 6 * MEMORY_HEADS)
    select = jnp.where(select, 1.0, 0.0).astype(BF16)
    rows_wait.wait()
    arrived(waits)
    arrived(extra_waits)
    for block in range(group):
        here = slice(block * count, (block + 1) * count)
        pre = None
        for place in range(held.shape[0]):
            wide = held.shape[3]
            start = 0 if held.shape[0] == 1 else pl.multiple_of((core if place == 0 else 1 - core) * wide, wide)
            term = dot_nt(rows_in[:, pl.ds(start, wide)], held[place, block])
            pre = term if pre is None else pre + term
        gates[:, here] = pre
        extras[:, here] = dot_nt(select, extra_in[block])
    width = gates.shape[1]

    def gate(kind):
        return gates[pl.ds(kind * MEMORY_HEADS + head, 1), :] + gate_bias[kind * MEMORY_HEADS + head]

    sub = lax.broadcasted_iota(jnp.int32, (8, width), 0)
    forget_f = log_sigmoid(gate(1)) + extras[pl.ds(head, 1), :]
    forget_b = log_sigmoid(gate(3)) + extras[pl.ds(MEMORY_HEADS + head, 1), :]
    decay_f = scan_lanes(jnp.broadcast_to(forget_f, (8, width)), jnp.add, 0.0, False)[0:1]
    decay_b = scan_lanes(jnp.broadcast_to(forget_b, (8, width)), jnp.add, 0.0, True)[0:1]
    level_f, level_b = gate(0) - decay_f, gate(2) - decay_b
    peak_f = scan_lanes(jnp.broadcast_to(level_f, (8, width)), jnp.maximum, LOW_START, False)[0:1]
    peak_b = scan_lanes(jnp.broadcast_to(level_b, (8, width)), jnp.maximum, LOW_START, True)[0:1]
    most_f = jnp.max(level_f, axis=1, keepdims=True)
    most_b = jnp.max(level_b, axis=1, keepdims=True)
    end_f, end_b = jnp.exp(level_f - most_f) * key_scale, jnp.exp(level_b - most_b) * key_scale
    vectors = [level_f, level_b, decay_f, decay_b, peak_f, peak_b, end_f, end_b]
    table = jnp.zeros((8, width), F32)
    for place, vector in enumerate(vectors):
        table = jnp.where(sub == place, vector, table)
    rows_out[...] = table


def front_kernel(dims, tab, *refs):
    group, blocks, rows, n_parts, n_pieces = dims
    parts, refs = refs[:n_parts], refs[n_parts:]
    pieces, gate_pieces, refs = refs[:n_pieces], refs[n_pieces : 2 * n_pieces], refs[2 * n_pieces :]
    glu_out, head_out, tail_out, held, value_w, gate_w, part_sems, sems = refs
    weight_waits = fetch_weights(tab, group, blocks, rows, pieces, (value_w,), sems.at[pl.ds(0, 1)])
    weight_waits += fetch_weights(tab, group, blocks, rows, gate_pieces, (gate_w,), sems.at[pl.ds(1, 1)])
    waits = fetch_parts(tab, parts, held, part_sems)
    arrived(weight_waits)
    arrived(waits)
    count = held.shape[2]
    for block in range(group):
        have = [held[place, block] for place in range(held.shape[0])]
        glu = (project(have, value_w) * jax.nn.sigmoid(project(have, gate_w))).astype(BF16)
        glu_out[block * count : (block + 1) * count, :] = glu
        if block == 0:
            head_out[...] = glu[0:HALO, :]
        if block == group - 1:
            tail_out[...] = glu[count - HALO :, :]


def states_kernel(dims, tab, *refs):
    group, blocks, rows, n_parts, n_pieces, quarters, n_sends = dims
    refs = list(refs)
    parts = [refs.pop(0) for _ in range(n_parts)]
    key_pieces = [refs.pop(0) for _ in range(n_pieces)]
    value_pieces = [refs.pop(0) for _ in range(n_pieces)]
    table_in, key_out, value_out = [refs.pop(0) for _ in range(3)]
    sends = [refs.pop(0) for _ in range(n_sends)]
    held, key_w, value_w, table, part_sems, sems = refs
    key_wait = fetch_weights(tab, group, blocks, rows, key_pieces, (key_w,), sems.at[pl.ds(0, 1)])
    value_wait = fetch_weights(tab, group, blocks, rows, value_pieces, (value_w,), sems.at[pl.ds(1, 1)])
    table_wait = fetch([(table_in, table, sems.at[2])])
    waits = fetch_parts(tab, parts, held, part_sems)
    arrived(key_wait)
    arrived(value_wait)
    arrived(table_wait)
    arrived(waits)
    count = held.shape[2]
    columns = jnp.transpose(table[...])
    mats, sums = [None, None], [None, None]
    for block in range(group):
        here = slice(block * count, (block + 1) * count)
        have = [held[place, block] for place in range(held.shape[0])]
        keys = project(have, key_w).astype(BF16)
        key_out[here, :] = keys
        values = project(have, value_w).astype(BF16)
        value_out[here, :] = values
        keys = keys.astype(F32)
        for place in range(2):
            weighted = keys * columns[here, 6 + place : 7 + place]
            line = jnp.sum(weighted, axis=0, keepdims=True)
            mat = dot_tn(weighted.astype(BF16), values)
            sums[place] = line if block == 0 else sums[place] + line
            mats[place] = mat if block == 0 else mats[place] + mat
    width = table.shape[1]
    at = lax.broadcasted_iota(jnp.int32, (TAIL, HEAD), 0)
    made = []
    for place, lane in ((0, width - 1), (1, 0)):
        total = table[2 + place : 3 + place, lane : lane + 1]
        most = table[4 + place : 5 + place, lane : lane + 1]
        lines = (*split3(sums[place]), *split3(total), *split3(total + most))
        tail = jnp.zeros((TAIL, HEAD), F32)
        for line, value in enumerate(lines):
            tail = jnp.where(at == line, value, tail)
        made.append((mats[place].astype(BF16), tail.astype(BF16)))
    for slot, send in enumerate(sends):
        if n_sends == quarters - 1 and quarters > 1:
            ahead = tab[3 * group] + slot + 1 < quarters
            for chosen, (mat, tail) in ((ahead, made[0]), (jnp.logical_not(ahead), made[1])):

                @pl.when(chosen)
                def _(mat=mat, tail=tail, send=send):
                    send[0:HEAD, :] = mat
                    send[HEAD:, :] = tail
        else:
            send[0:HEAD, :] = made[slot][0]
            send[HEAD:, :] = made[slot][1]


def local_kernel(dims, tab, *refs):
    group, blocks, rows, n_parts, n_pieces, key_scale = dims
    parts, pieces = refs[:n_parts], refs[n_parts : n_parts + n_pieces]
    keys_in, values_in, table_in = refs[n_parts + n_pieces : n_parts + n_pieces + 3]
    query_out, numer_f, numer_b, denom_out = refs[n_parts + n_pieces + 3 : n_parts + n_pieces + 7]
    held, query_w, keys, values, table, part_sems, sems = refs[n_parts + n_pieces + 7 :]
    weight_wait = fetch_weights(tab, group, blocks, rows, pieces, (query_w,), sems.at[pl.ds(3, 1)], True)
    waits = fetch_parts(tab, parts, held, part_sems)
    others_wait = fetch(
        [(keys_in, keys, sems.at[0]), (values_in, values, sems.at[1]), (table_in, table, sems.at[2])]
    )
    arrived(weight_wait)
    arrived(waits)
    length = keys.shape[0]
    count = length // group
    spot_t = lax.broadcasted_iota(jnp.int32, (count, count), 0)
    spot_s = lax.broadcasted_iota(jnp.int32, (count, count), 1)
    masks = (spot_s <= spot_t, spot_s >= spot_t)
    lane = lax.broadcasted_iota(jnp.int32, (count, 128), 1)
    for block in range(group):
        here = slice(block * count, (block + 1) * count)
        queries = project([held[place, block] for place in range(held.shape[0])], query_w).astype(BF16)
        query_out[here, :] = queries
        if block == 0:
            arrived(others_wait)
        raw = dot_nt(queries, keys[...]) * key_scale
        columns = jnp.transpose(table[:, here])
        denoms = []
        for way, out in enumerate((numer_f, numer_b)):
            top = columns[:, 4 + way : 5 + way]
            power = jnp.where(masks[way], table[way : way + 1, here] - top, LOW_START)
            scores = raw[:, here] * jnp.exp(power)
            denom = jnp.sum(scores, axis=1, keepdims=True)
            numer = dot(scores.astype(BF16), values[here, :])
            others = slice(0, block * count) if way == 0 else slice((block + 1) * count, length)
            if others.stop > others.start:
                scores = raw[:, others] * jnp.exp(table[way : way + 1, others] - top)
                denom = denom + jnp.sum(scores, axis=1, keepdims=True)
                numer = numer + dot(scores.astype(BF16), values[others, :])
            out[here, :] = numer.astype(BF16)
            denoms.append(denom)
        denom_out[here, :] = jnp.where(lane == 0, denoms[0], denoms[1])


def conv_kernel(tab, glu, before, after, taps, conv_out, stats_out, padded, sums):
    length, width = glu.shape
    padded[0:HALO, :] = before[...].astype(F32)
    padded[HALO : HALO + length, :] = glu[...].astype(F32)
    padded[HALO + length :, :] = after[...].astype(F32)
    chunk = 64
    lead = HALO - REACH
    lane = lax.broadcasted_iota(jnp.int32, (chunk, 128), 1)

    def one(step, carry):
        base = pl.multiple_of(step * chunk, chunk)
        line = jnp.zeros((chunk, 128), F32)
        square = jnp.zeros((chunk, 128), F32)
        for left in range(0, width, 128):
            lanes = slice(left, left + 128)
            total = jnp.zeros((chunk, 128), F32)
            window_all = padded[pl.ds(base, chunk + 32), lanes]
            for shift in range(8):
                window = pltpu.roll(window_all, chunk + 32 - shift, 0) if shift else window_all
                for high in range(4):
                    tap = 8 * high + shift - lead
                    if 0 <= tap < KW:
                        total = total + taps[tap : tap + 1, lanes] * window[8 * high : 8 * high + chunk, :]
            conv_out[pl.ds(base, chunk), lanes] = total
            line = line + total
            square = square + total * total
        line = jnp.sum(line, axis=1, keepdims=True)
        square = jnp.sum(square, axis=1, keepdims=True)
        sums[pl.ds(base, chunk), :] = jnp.where(lane == 0, line, square)
        return carry

    lax.fori_loop(0, length // chunk, one, 0)
    stats_out[...] = jnp.transpose(sums[...])[0:8, :]


def act_kernel(dims, tab, conv, *refs):
    group, channels, halves = dims
    stats, (gain, bias), outs = refs[:group], refs[group : group + 2], refs[group + 2 :]
    total = stats[0][...]
    for more in stats[1:]:
        total = total + more[...]
    mean = total[0:1, :] / channels
    var = total[1:2, :] / channels - mean * mean
    scale = lax.rsqrt(var + EPS)
    sub = lax.broadcasted_iota(jnp.int32, total.shape, 0)
    columns = jnp.transpose(jnp.where(sub == 0, mean, scale))
    count = outs[0].shape[0]
    for slot, out in enumerate(outs):
        which = tab[group + slot]
        start = pl.multiple_of(which * count, count)
        picked = columns[0:count, :]
        for block in range(1, group):
            picked = jnp.where(which == block, columns[block * count : (block + 1) * count, :], picked)
        normal = (conv[pl.ds(start, count), :] - picked[:, 0:1]) * picked[:, 1:2]
        normal = normal * gain[...] + bias[...]
        place_rows(tab, group, halves, out, (normal * jax.nn.sigmoid(normal)).astype(BF16))


def place_rows(tab, group, halves, out, value):
    if halves == 1:
        out[...] = value
        return
    half = value.shape[0] // 2
    own = tab[3 * group + 2]
    out[pl.ds(pl.multiple_of((1 - own) * half, half), half), :] = value[:half, :]
    out[pl.ds(pl.multiple_of(own * half, half), half), :] = value[half:, :]


def incoming(pieces):
    levels, best, passed = [], jnp.full((1, HEAD), LOW_START, F32), jnp.zeros((1, HEAD), F32)
    for piece, there in pieces:
        lines = piece[HEAD:, :].astype(F32)
        level = lines[6:7] + lines[7:8] + lines[8:9] + passed
        if there is not None:
            level = jnp.where(there, level, LOW_START)
        levels.append(level)
        best = jnp.maximum(best, level)
        passed = passed + lines[3:4] + lines[4:5] + lines[5:6]
    mat, vec = jnp.zeros((HEAD, HEAD), F32), jnp.zeros((1, HEAD), F32)
    for (piece, there), level in zip(pieces, levels):
        weight = jnp.exp(level - best)
        if there is not None:
            weight = jnp.where(there, weight, 0.0)
        lines = piece[HEAD:, :].astype(F32)
        mat = mat + weight * piece[0:HEAD, :].astype(F32)
        vec = vec + weight * (lines[0:1] + lines[1:2] + lines[2:3])
    return mat, vec, best


def finish_kernel(dims, tab, *refs):
    group, n_states, ringed, halves = dims
    queries_in, numer_f, numer_b, denoms_in, table_in = refs[:5]
    states_in, gain = refs[5 : 5 + n_states], refs[5 + n_states]
    outs = refs[6 + n_states : 6 + n_states + group]
    states, table, queries_all, numers, denoms_all, result, sems, block_sems = refs[6 + n_states + group :]
    length = queries_in.shape[0]
    count = length // group
    first = fetch(
        [(state, states.at[slot], sems.at[slot]) for slot, state in enumerate(states_in)]
        + [(table_in, table, sems.at[n_states])]
    )
    waits = []
    for block in range(group):
        here = pl.ds(block * count, count)
        waits.append(
            fetch(
                [
                    (queries_in.at[here, :], queries_all.at[here, :], block_sems.at[block, 0]),
                    (numer_f.at[here, :], numers.at[0, here, :], block_sems.at[block, 1]),
                    (numer_b.at[here, :], numers.at[1, here, :], block_sems.at[block, 2]),
                    (denoms_in.at[here, :], denoms_all.at[here, :], block_sems.at[block, 3]),
                ]
            )
        )
    arrived(first)
    pieces = [states.at[slot] for slot in range(n_states)]
    if ringed:
        at = tab[3 * group]
        ahead = [(state, slot + 1 <= at) for slot, state in enumerate(pieces)]
        back = [(state, slot + 1 > at) for slot, state in enumerate(pieces)][::-1]
    else:
        ahead, back = [(pieces[0], None)], [(pieces[1], None)]
    mats, vecs, bests = [], [], []
    for these in (ahead, back):
        mat, vec, best = incoming(these)
        mats.append(mat.astype(BF16))
        vecs.append(vec)
        bests.append(best[:, 0:1])
    line = lax.broadcasted_iota(jnp.int32, (128, HEAD), 0)
    vec = jnp.where(line == 0, vecs[0], vecs[1])
    vec_high = vec.astype(BF16)
    vec_low = (vec - vec_high.astype(F32)).astype(BF16)
    sub = lax.broadcasted_iota(jnp.int32, (8, length), 0)
    peak = jnp.where(sub == 0, table[4:5, :], table[5:6, :])
    decay = jnp.where(sub == 0, table[2:3, :], table[3:4, :])
    best = jnp.where(sub == 0, bests[0], bests[1])
    top = jnp.maximum(peak, best)
    carry = jnp.transpose(jnp.exp(best - top))
    stay = jnp.transpose(jnp.exp(peak - top))
    floor = jnp.transpose(jnp.exp(-(decay + top)))
    for block in range(group):
        here = slice(block * count, (block + 1) * count)
        arrived(waits[block])
        queries = queries_all[here, :]
        along = (dot_nt(queries, vec_high) + dot_nt(queries, vec_low))[:, 0:8]
        denom = stay[here, :] * denoms_all[here, 0:8] + carry[here, :] * along
        inverse = 1.0 / jnp.maximum(jnp.abs(denom), floor[here, :])
        left, right = stay[here, :] * inverse, carry[here, :] * inverse
        summed = None
        for way, mat in enumerate(mats):
            term = left[:, way : way + 1] * numers[way, here, :].astype(F32)
            term = term + right[:, way : way + 1] * dot(queries, mat)
            summed = term if summed is None else summed + term
        scale = lax.rsqrt(jnp.mean(summed * summed, axis=1, keepdims=True) + EPS)
        result[here, :] = (summed * scale * gain[...]).astype(BF16)
    for slot, out in enumerate(outs):
        start = pl.multiple_of(tab[group + slot] * count, count)
        place_rows(tab, group, halves, out, result[pl.ds(start, count), :])


def compose_line(total, level, mat, vec):
    tail = jnp.concatenate([jnp.broadcast_to(x[None, :], (1, HEAD)) for x in (*split3(vec), *split3(total + jnp.zeros((HEAD,), F32)), *split3(level + jnp.zeros((HEAD,), F32)))])
    tail = jnp.concatenate([tail, jnp.zeros((TAIL - tail.shape[0], HEAD), F32)])
    return jnp.concatenate([mat, tail]).astype(BF16)


def shards(
    tokens,
    norm_gain,
    glu_value,
    glu_gate,
    conv_taps,
    ln_gain,
    ln_bias,
    query_weight,
    key_weight,
    value_weight,
    gate_weight,
    gate_bias,
    log_decay_extra,
    mem_gain,
    out_conv,
    out_mem,
):
    sp, tp = lax.axis_size("sp"), lax.axis_size("tp")
    group = mem_gain.shape[0] // HEAD
    quarters = sp // group
    count = tokens.shape[0]
    length = group * count
    rows = key_weight.shape[0]
    features = norm_gain.shape[0]
    channels = conv_taps.shape[1] // group
    conv_all = channels * group * tp
    blocks = sp
    key_scale = HEAD ** (-0.5)
    me, core = lax.axis_index("sp"), lax.axis_index("tp")
    place, quarter = me % group, me // group
    paired = tp == 2
    even = group & (group - 1) == 0
    ringed = quarters <= RING_MOST

    def source(p, slot):
        return p ^ slot if even else (p - slot) % group

    def target(p, slot):
        return p ^ slot if even else (p + slot) % group

    def in_plane(x, slot):
        if slot == 0:
            return x
        pairs = [(i, i - i % group + target(i % group, slot)) for i in range(sp)]
        return lax.ppermute(x, "sp", pairs)

    def along(x, hops, ring=False):
        pairs = [(i, i + hops * group) for i in range(sp)]
        pairs = [(i, j % sp) for i, j in pairs] if ring else [(i, j) for i, j in pairs if 0 <= j < sp]
        return lax.ppermute(x, "sp", pairs)

    def swap(x):
        return lax.ppermute(x, "tp", [(0, 1), (1, 0)])

    lines = [[k * group + j for k in range(quarters)] for j in range(group)]

    def tall(x):
        return jnp.concatenate(x, axis=0) if len(x) > 1 else x[0]

    def split_weights(weights, width):
        got = []
        for slot in range(group):
            to = target(place, slot) * width
            sent = tall([lax.dynamic_slice_in_dim(weight, to, width, 1) for weight in weights])
            got.append(in_plane(sent, slot))
        return got

    def ring(piece):
        if not ringed:
            return [lax.all_gather(piece, "sp", axis=0, tiled=True, axis_index_groups=lines)]
        pieces = [piece]
        for _ in range(1, quarters):
            pieces.append(along(pieces[-1], 1, True))
        return pieces

    slots = list(range(group))
    sources = [source(place, slot) for slot in slots]
    targets = [target(place, slot) for slot in slots]
    inverse = [p ^ place if even else (place - p) % group for p in slots]
    shift = core * tokens.shape[1] if paired else 0
    offsets = []
    for hop in range(quarters):
        block_quarter = (quarter - hop) % quarters if ringed else hop
        for slot in slots:
            offsets.append(((block_quarter * group + sources[slot]) * rows - shift) % features)
    head = core * group + place
    entries = (*sources, *targets, *inverse, quarter, 0, core, place, head, *offsets)
    tab = jnp.stack([jnp.asarray(x, jnp.int32) for x in entries])

    glu_piece = tall(split_weights([glu_value], channels))
    gate_piece = tall(split_weights([glu_gate], channels))
    key_piece = tall(split_weights([key_weight], HEAD))
    wide = tokens.astype(F32)
    squares = jnp.sum(wide * wide, axis=-1, keepdims=True)
    squares = squares + swap(squares) if paired else lax.psum(squares, "tp")
    own_gain = lax.dynamic_slice_in_dim(norm_gain, core * tokens.shape[1], tokens.shape[1], 0)
    normed = (wide * lax.rsqrt(squares / features + EPS) * own_gain).astype(BF16)
    extras = [part.astype(BF16) for part in split3(log_decay_extra)]
    extras = jnp.pad(jnp.concatenate(extras, 1), ((0, 0), (0, 128 - 3 * 2 * MEMORY_HEADS)))
    own_width = tokens.shape[1]
    payload = jnp.concatenate([normed, extras], 1)
    payloads = [in_plane(payload, slot) for slot in slots]
    if paired:
        parts = payloads + [swap(x) for x in payloads]
        extra, extra_at, part_width = payloads, own_width // 128, own_width
    else:
        parts = [lax.all_gather(x[:, :own_width], "tp", axis=1, tiled=True) for x in payloads]
        extra, extra_at, part_width = [x[:, own_width:] for x in payloads], 0, features
    glu_pieces = ring(glu_piece)
    gate_pieces = ring(gate_piece)
    value_piece = tall(split_weights([value_weight], HEAD))
    conv_rows = tall([lax.dynamic_slice_in_dim(out_conv, at * channels, channels, 0) for at in sources])
    mem_rows = tall([lax.dynamic_slice_in_dim(out_mem, at * HEAD, HEAD, 0) for at in sources])
    key_pieces = ring(key_piece)
    value_pieces = ring(value_piece)
    query_rows = ring(query_weight)
    query_cuts = []
    for held_rows in query_rows:
        query_cuts.append([lax.dynamic_slice_in_dim(held_rows, to * HEAD, HEAD, 1) for to in targets])
    query_pieces = []
    for slot in slots:
        sent = [cut[slot] for cut in query_cuts]
        query_pieces.append(in_plane(tall(sent), slot))

    def far(arrays):
        return [pl.BlockSpec(memory_space=pl.ANY) for _ in arrays]

    def wholes(shapes):
        return [whole(x.shape) for x in shapes]

    def dma(*dims):
        return pltpu.SemaphoreType.DMA(dims)

    def call(kernel, in_specs, out_specs, out_shape, scratch, flops, steps=1):
        return pl.pallas_call(
            kernel,
            grid_spec=pltpu.PrefetchScalarGridSpec(
                num_scalar_prefetch=1,
                grid=(steps,),
                in_specs=in_specs,
                out_specs=out_specs,
                scratch_shapes=scratch,
            ),
            out_shape=out_shape,
            compiler_params=params(),
            cost_estimate=pl.CostEstimate(flops=flops, transcendentals=0, bytes_accessed=4 << 20),
        )

    def shape(dims, kind=BF16):
        return jax.ShapeDtypeStruct(dims, kind)

    n_parts, n_pieces = len(parts), len(key_pieces)
    halves = 2 if paired else 1
    work = 2 * length * features * HEAD
    held = [pltpu.VMEM((n_parts // group, group, count, part_width), BF16)]
    part_sems = [dma(n_parts)]
    square = [pltpu.VMEM((features, HEAD), BF16)]
    table = call(
        functools.partial(gates_kernel, (group, n_parts, extra_at, key_scale)),
        far(parts) + far(extra) + far([gate_weight]) + [pl.BlockSpec(memory_space=pltpu.SMEM)],
        whole((8, length)),
        shape((8, length), F32),
        held
        + [pltpu.VMEM((group, count, 128), BF16), pltpu.VMEM((4 * MEMORY_HEADS, features), BF16)]
        + [pltpu.VMEM((4 * MEMORY_HEADS, length), F32), pltpu.VMEM((2 * MEMORY_HEADS, length), F32)]
        + part_sems
        + [dma(group + 1)],
        work,
    )(tab, *parts, *extra, gate_weight.T, gate_bias)

    made = [shape((length, channels)), shape((HALO, channels)), shape((HALO, channels))]
    glu, glu_head, glu_tail = call(
        functools.partial(front_kernel, (group, blocks, rows, n_parts, n_pieces)),
        far(parts) + far(glu_pieces) + far(gate_pieces),
        wholes(made),
        made,
        held + [pltpu.VMEM((features, channels), BF16)] * 2 + part_sems + [dma(2)],
        2 * work,
    )(tab, *parts, *glu_pieces, *gate_pieces)

    glu_before = along(glu_tail, 1)
    glu_after = along(glu_head, -1)

    def own_lanes(lines, width):
        return pl.BlockSpec((lines, width), lambda i, tab: (0, tab[3 * group + 3]))

    conv, stats = call(
        conv_kernel,
        [whole((length, channels)), whole((HALO, channels)), whole((HALO, channels)), own_lanes(KW, channels)],
        [whole((length, channels)), whole((8, length))],
        [shape((length, channels), F32), shape((8, length), F32)],
        [pltpu.VMEM((length + 2 * HALO, channels), F32), pltpu.VMEM((length, 128), F32)],
        2 * work,
        1,
    )(tab, glu, glu_before, glu_after, conv_taps)
    stats = stats + swap(stats) if paired else lax.psum(stats, "tp")
    all_stats = [in_plane(stats, slot) for slot in slots]
    acts = call(
        functools.partial(act_kernel, (group, conv_all, halves)),
        [whole((length, channels))] + [whole((8, length))] * group + [own_lanes(1, channels)] * 2,
        [whole((count, channels))] * group,
        [shape((count, channels))] * group,
        [],
        work,
        1,
    )(tab, conv, *all_stats, ln_gain[None, :], ln_bias[None, :])
    acts = [in_plane(act, slot) for slot, act in enumerate(acts)]

    n_sends = quarters - 1 if ringed else 2
    made = [shape((length, HEAD))] * 2 + [shape((HEAD + TAIL, HEAD))] * n_sends
    keys, values, *sends = call(
        functools.partial(states_kernel, (group, blocks, rows, n_parts, n_pieces, quarters, n_sends)),
        far(parts) + far(key_pieces) + far(value_pieces) + far([table]),
        wholes(made),
        made,
        held + square * 2 + [pltpu.VMEM((8, length), F32)] + part_sems + [dma(3)],
        2 * work,
    )(tab, *parts, *key_pieces, *value_pieces, table)
    if ringed:
        states = [along(send, hop + 1, True) for hop, send in enumerate(sends)]
    else:
        states = far_states(sends[0], sends[1], quarter, quarters, lines)

    tall_head = [pltpu.VMEM((length, HEAD), BF16)]
    made = [shape((length, HEAD))] * 3 + [shape((length, 128), F32)]
    locals_made = call(
        functools.partial(local_kernel, (group, blocks, rows, n_parts, len(query_pieces), key_scale)),
        far(parts) + far(query_pieces) + far([keys, values, table]),
        wholes(made),
        made,
        held + square + tall_head * 2 + [pltpu.VMEM((8, length), F32)] + part_sems + [dma(4)],
        work,
    )(tab, *parts, *query_pieces, keys, values, table)

    made = [shape((count, HEAD))] * group
    memories = call(
        functools.partial(finish_kernel, (group, len(states), ringed, halves)),
        far(locals_made) + far([table]) + far(states) + [own_lanes(1, HEAD)],
        wholes(made),
        made,
        [pltpu.VMEM((len(states), HEAD + TAIL, HEAD), BF16), pltpu.VMEM((8, length), F32)]
        + tall_head
        + [pltpu.VMEM((2, length, HEAD), BF16), pltpu.VMEM((length, 128), F32)]
        + tall_head
        + [dma(len(states) + 1), dma(group, 4)],
        work,
    )(tab, *locals_made, table, *states, mem_gain[None, :])
    memories = [in_plane(memory, slot) for slot, memory in enumerate(memories)]

    partial = lax.optimization_barrier(dot(jnp.concatenate(acts, 1), conv_rows))
    result = (partial + dot(jnp.concatenate(memories, 1), mem_rows)).astype(BF16)
    if paired:
        half = count // 2
        return (result[half:].astype(F32) + swap(result[:half]).astype(F32)).astype(BF16)
    return lax.psum_scatter(result, "tp", scatter_dimension=0, tiled=True)


def far_states(state_f, state_b, quarter, quarters, lines):
    found = []
    for state, reverse in ((state_f, False), (state_b, True)):
        pieces = lax.all_gather(state, "sp", axis_index_groups=lines).astype(F32)
        if reverse:
            pieces = jnp.flip(pieces, 0)
        at = quarters - 1 - quarter if reverse else quarter
        totals = pieces[:, HEAD + 3, 0] + pieces[:, HEAD + 4, 0] + pieces[:, HEAD + 5, 0]
        levels = pieces[:, HEAD + 6, 0] + pieces[:, HEAD + 7, 0] + pieces[:, HEAD + 8, 0]
        order = jnp.arange(quarters)
        between = (order[None, :] > order[:, None]) & (order[None, :] < at)
        levels = levels + jnp.sum(jnp.where(between, totals[None, :], 0.0), axis=1)
        levels = jnp.where(order < at, levels, LOW_START)
        best = jnp.max(levels)
        weights = jnp.exp(levels - best)
        mat = jnp.sum(weights[:, None, None] * pieces[:, :HEAD], axis=0)
        vec = jnp.sum(weights[:, None] * (pieces[:, HEAD] + pieces[:, HEAD + 1] + pieces[:, HEAD + 2]), axis=0)
        found.append(compose_line(jnp.zeros((), F32), best, mat, vec))
    return found


def solution(mesh):
    in_specs = (
        P("sp", "tp"),
        P(),
        P("sp", "tp"),
        P("sp", "tp"),
        P(None, "tp"),
        P("tp"),
        P("tp"),
        P("sp", "tp"),
        P("sp", "tp"),
        P("sp", "tp"),
        P(),
        P(),
        P("sp", None),
        P("tp"),
        P("tp", None),
        P("tp", None),
    )
    out_specs = P(("sp", "tp"), None)

    return jax.shard_map(shards, mesh=mesh, in_specs=in_specs, out_specs=out_specs, check_vma=False)
```
